256 devices in a mesh: ep: 64 (over z, x, core), tp: 4 (over y).
Axes of the slice: x: 4, y: 4, z: 8, core: 2. Of those that a mesh axis runs over, the one named last changes fastest.
Arguments:
- conv_input: bfloat16 [65536, 2048], P('ep', 'tp'), may hold values from -6 to 6
- conv_kernel: bfloat16 [31, 2048], P(None, 'tp'), may hold values from -2 to 2
- norm_gain: float32 [2048], P('tp'), may hold values from 0.1 to 1.9
- norm_shift: float32 [2048], P('tp'), may hold values from -3 to 3
- conv_proj: bfloat16 [2048, 2048], P('tp'), may hold values from -0.125 to 0.125
- moe_input: bfloat16 [16384, 2048], P(('ep', 'tp')), may hold values from -6 to 6
- moe_gain: float32 [2048], replicated, may hold values from 0.1 to 1.9
- routes: int32 [16384, 2], P('ep'), may hold values from 0 to 63, all different within a row; in each aligned block of 256 rows (0 to 255, 256 to 511, ...) at most 16 rows name the same one
- route_weights: float32 [16384, 2], P('ep'), may hold values from 0.2 to 1
- gate_proj: bfloat16 [64, 2048, 2048], P('ep', None, 'tp'), may hold values from -0.125 to 0.125
- up_proj: bfloat16 [64, 2048, 2048], P('ep', None, 'tp'), may hold values from -0.125 to 0.125
- down_proj: bfloat16 [64, 2048, 2048], P('ep', 'tp'), may hold values from -0.125 to 0.125
Outputs:
- conv_out: bfloat16 [65536, 2048], P(('ep', 'tp'))
- moe_out: bfloat16 [16384, 2048], P(('ep', 'tp'))
The draws below stay inside these ranges and needn't reach their ends.
Inputs may be any that keep to these rules, and one draw needn't show every extreme that they name: `routes`: each row names 2 different experts. In each aligned block of 256 rows no expert is named by more than 16 rows, and in some blocks an expert is named by exactly 16 rows.
All inputs are finite; a program needn't handle non-finite values.
Results may differ from the reference program's by a relative error of at most 0.012.
Values may be sent and summed in bfloat16 or wider, within the bound.
A program may use at most 128 MiB of HBM per device.

```python
import math
import jax
import jax.numpy as jnp
import numpy as np
from jax import lax

D = 2048
FE = 2048
CONV_WIDTH = 31
TOPK = 2
TOK_DEV = 64
EXPERTS = 64
CAPG = 16
CONV_TOKENS = 65536
MOE_TOKENS = 16384
N_EP = 64
N_TP = 4


def draw_conv_kernel(key, part):
    first_key, second_key = jax.random.split(jax.random.fold_in(key, 11))
    factors = jax.random.permutation(first_key, jnp.array([0.5, 0.9, 1.6, 2.6], jnp.float32))
    channel_block = jnp.arange(D, dtype=jnp.int32) * 4 // D
    column_scale = factors[channel_block] / math.sqrt(CONV_WIDTH)
    base = jnp.clip(jax.random.normal(second_key, (CONV_WIDTH, D), jnp.float32), -4.0, 4.0)
    return (base * column_scale[None, :]).astype(jnp.bfloat16)


def shard_levels(stream_key, extent, cuts, least, top_value):
    def one(axis_at, parts):
        heights = jax.random.uniform(jax.random.fold_in(jax.random.fold_in(stream_key, 6), axis_at), (parts,), jnp.float32, least / len(cuts), top_value / len(cuts))
        return jnp.repeat(jnp.exp(heights), extent[axis_at] // parts).reshape((-1,) + (1,) * (len(extent) - axis_at - 1))

    factor_of = one(*cuts[0])
    for cut in cuts[1:]:
        factor_of = factor_of * one(*cut)
    return factor_of


def assign_block(own_key, own, number, rows, number_of, top, most, slope):
    ranking = jax.random.permutation(own_key, number_of)
    packed, usual = load_shares(number_of, rows * top, most, slope, True), load_shares(number_of, rows * top, most, slope, False)
    places = jnp.arange(number_of)

    def named(sizes, offset_by):
        used = int((sizes > 0).sum())
        fixed = max(1, used // 4)
        moved = fixed + (places - fixed + offset_by * (used - fixed)) % max(1, number_of - fixed)
        return jnp.zeros((number_of,), jnp.int32).at[ranking[jnp.where(places < fixed, places, moved)]].set(jnp.asarray(sizes, jnp.int32))

    sizes = jnp.where(number % 4 == 0, named(packed, number // 4), named(usual, number - number // 4 - 1))
    mixed = jax.random.permutation(jax.random.fold_in(own, 3), number_of)
    giver, taker = mixed[0:number_of // 2 * 2:2], mixed[1:number_of // 2 * 2:2]
    slack = jnp.minimum(sizes[giver] - 1, most - sizes[taker]) // 2
    slack = jnp.where((giver == ranking[0]) | (taker == ranking[0]) | (sizes[taker] == 0), 0, jnp.maximum(slack, 0))
    moved = jax.random.randint(jax.random.fold_in(own, 4), (number_of // 2,), 0, 1 << 20) % (slack + 1)
    sizes = sizes.at[giver].add(-moved).at[taker].add(moved)
    labels = jnp.searchsorted(jnp.cumsum(sizes), jnp.arange(rows * top), side="right").astype(jnp.int32)
    listing = labels.reshape(top, rows).T
    listing = listing[jax.random.permutation(jax.random.fold_in(own, 1), rows)]
    offset_by = jax.random.randint(jax.random.fold_in(own, 2), (rows, 1), 0, top)
    return jnp.take_along_axis(listing, (jnp.arange(top)[None, :] + offset_by) % top, axis=1)


def load_shares(amount, total, most, slope, full):
    portions = [(1 << 20) // math.isqrt(standing ** slope) + 1 for standing in range(1, amount + 1)]
    largest = most if full else min(most, max(-(-total // amount), total * portions[0] // sum(portions)))
    least = 1 if total - largest >= amount - 1 else 0
    counts, rest = [largest] + [least] * (amount - 1), total - largest - least * (amount - 1)
    while rest > 0:
        candidates = [i for i in range(1, amount) if counts[i] < largest] or [i for i in range(1, amount) if counts[i] < most]
        whole, left = sum([portions[i] for i in candidates]), rest
        for i in candidates:
            more = min(most - counts[i], max(1, left * portions[i] // whole), rest)
            counts[i] = counts[i] + more
            rest = rest - more
    return np.array(counts)


def noise(stream_key, extent, scale, limit, cuts=(), held_as=jnp.bfloat16):
    gain = shard_levels(stream_key, extent, cuts, -0.22, 0.18) if cuts else 1.0
    entries = jax.random.normal(stream_key, extent, jnp.float32) * scale * gain
    return jnp.minimum(jnp.maximum(entries, -limit), limit).astype(held_as)


def setup_inputs(seed: int = 0) -> dict:
    splits = jax.random.split(jax.random.key(seed), 13)
    conv_input = noise(splits[0], (CONV_TOKENS, D), 1.0, 6.0, ((0, 64), (1, 4)))
    conv_kernel = draw_conv_kernel(jax.random.fold_in(splits[12], 71), 0)
    norm_gain = jnp.clip(1.0 + 0.18 * jax.random.normal(splits[2], (D,), jnp.float32), 0.1, 1.9)
    norm_shift = noise(splits[3], (D,), 0.5, 3.0, ((0, 4),), jnp.float32)
    conv_proj = noise(splits[4], (D, D), D ** -0.5, 0.125, ((0, 4),))
    moe_input = noise(splits[5], (MOE_TOKENS, D), 1.0, 6.0, ((0, 256),))
    moe_gain = jnp.clip(1.0 + 0.18 * jax.random.normal(splits[6], (D,), jnp.float32), 0.1, 1.9)
    routes_keys = jax.random.split(jax.random.fold_in(splits[7], 1), MOE_TOKENS // (N_TP * TOK_DEV))
    routes_turns = jax.random.permutation(jax.random.fold_in(splits[7], 3), MOE_TOKENS // (N_TP * TOK_DEV))
    routes = jax.vmap(lambda own, number: assign_block(jax.random.fold_in(splits[7], 2), own, number, N_TP * TOK_DEV, EXPERTS, TOPK, CAPG, 2))(routes_keys, routes_turns).reshape((MOE_TOKENS, TOPK))
    route_weights = jnp.clip(0.2 + 0.8 * jax.random.uniform(splits[8], (MOE_TOKENS, TOPK), jnp.float32) ** shard_levels(splits[8], (MOE_TOKENS, TOPK), ((0, 64),), -0.2, 0.2), 0.2, 1.0)
    gate_proj = noise(splits[9], (EXPERTS, D, FE), D ** -0.5, 0.125, ((0, 64), (2, 4)))
    up_proj = noise(splits[10], (EXPERTS, D, FE), D ** -0.5, 0.125, ((0, 64), (2, 4)))
    down_proj = noise(splits[11], (EXPERTS, FE, D), FE ** -0.5, 0.125, ((0, 64), (1, 4)))
    return dict(conv_input=conv_input, conv_kernel=conv_kernel, norm_gain=norm_gain, norm_shift=norm_shift, conv_proj=conv_proj, moe_input=moe_input, moe_gain=moe_gain, routes=routes, route_weights=route_weights, gate_proj=gate_proj, up_proj=up_proj, down_proj=down_proj)


def conv_half(conv_input, conv_kernel, norm_gain, norm_shift, conv_proj):
    reach = CONV_WIDTH - 1
    padded = jnp.concatenate([jnp.zeros((reach, D), conv_input.dtype), conv_input], axis=0)
    taps = conv_kernel.astype(jnp.float32)
    mixed = jnp.zeros((CONV_TOKENS, D), jnp.float32)
    for offset in range(CONV_WIDTH):
        mixed = mixed + padded[offset:offset + CONV_TOKENS].astype(jnp.float32) * taps[offset]
    center = lax.optimization_barrier(jnp.sum(mixed, axis=1)) / D
    spread = jnp.maximum(lax.optimization_barrier(jnp.sum(mixed * mixed, axis=1)) / D - center * center, 0.0)
    scaled = (mixed - center[:, None]) * lax.rsqrt(spread[:, None] + 1e-05) * norm_gain + norm_shift
    activated = jax.nn.silu(scaled).astype(jnp.bfloat16)
    block = D // N_TP
    total = jnp.zeros((CONV_TOKENS, D), jnp.float32)
    for part in range(N_TP):
        piece = jnp.dot(activated[:, part * block:(part + 1) * block], conv_proj[part * block:(part + 1) * block], preferred_element_type=jnp.float32)
        total = total + lax.optimization_barrier(piece.astype(jnp.bfloat16)).astype(jnp.float32)
    return total.astype(jnp.bfloat16)

def moe_half(moe_input, moe_gain, routes, route_weights, gate_proj, up_proj, down_proj):
    moe_float = moe_input.astype(jnp.float32)
    normed = (moe_float * lax.rsqrt(lax.optimization_barrier(jnp.mean(moe_float * moe_float, axis=1, keepdims=True)) + 1e-06) * moe_gain).astype(jnp.bfloat16)
    block = FE // N_TP
    slots = N_EP * CAPG

    def one_expert(total, items):
        expert, gate_w, up_w, down_w = items
        hits = routes == expert
        weight = lax.optimization_barrier(jnp.sum(jnp.where(hits, route_weights, 0.0), axis=1))
        named = jnp.any(hits, axis=1)
        index = jnp.nonzero(named, size=slots, fill_value=0)[0].astype(jnp.int32)
        valid = jnp.arange(slots, dtype=jnp.int32) < jnp.sum(named.astype(jnp.int32))
        rows = normed[index]
        result = jnp.zeros((slots, D), jnp.float32)
        for part in range(N_TP):
            low = part * block
            gated = jax.nn.silu(jnp.dot(rows, gate_w[:, low:low + block], preferred_element_type=jnp.float32))
            hidden = (gated * jnp.dot(rows, up_w[:, low:low + block], preferred_element_type=jnp.float32)).astype(jnp.bfloat16)
            piece = jnp.dot(hidden, down_w[low:low + block], preferred_element_type=jnp.float32)
            result = result + lax.optimization_barrier(piece.astype(jnp.bfloat16)).astype(jnp.float32)
        scale = jnp.where(valid, weight[index], 0.0)
        return (total.at[index].add(result * scale[:, None]), None)
    experts = jnp.arange(EXPERTS, dtype=jnp.int32)
    total, _ = lax.scan(one_expert, jnp.zeros((MOE_TOKENS, D), jnp.float32), (experts, gate_proj, up_proj, down_proj))
    return total.astype(jnp.bfloat16)

def reference(conv_input, conv_kernel, norm_gain, norm_shift, conv_proj, moe_input, moe_gain, routes, route_weights, gate_proj, up_proj, down_proj):
    conv_out = conv_half(conv_input, conv_kernel, norm_gain, norm_shift, conv_proj)
    moe_out = moe_half(moe_input, moe_gain, routes, route_weights, gate_proj, up_proj, down_proj)
    return (conv_out, moe_out)
```

```python
import functools

import jax
import jax.numpy as jnp
from jax import lax
from jax.experimental import pallas as pl
from jax.experimental.pallas import tpu as pltpu
from jax.sharding import PartitionSpec as P

MESH = pl.DeviceIdType.MESH
DIMS = (8, 4, 2)
f32, bf16, i32 = jnp.float32, jnp.bfloat16, jnp.int32


def layer(
    moe_in, moe_gain, routes, weights, taps_in, gain, shift, conv_hbm, proj_hbm, gate_hbm, up_hbm, down_hbm,
    conv_out, moe_out,
    padded, taps, mixed, sums, stats, stats_in, columns, proj, partial,
    conv_a, conv_b, conv_c, conv_d, conv_u, conv_v, history,
    gate, up, down, own, group, ranks, held_w, scale, outgoing, arrived, pieces,
    moe_a, moe_b, moe_c, moe_d, moe_u, moe_v, back_out, returned, combined, final,
    load_sem, hist_send, hist_recv, stat_send, stat_recv, a2a_send, a2a_recv, ep_send, ep_recv,
    gather_send, gather_recv, ret_send, ret_recv, back_send, back_recv, conv_send, conv_recv, fin_send, fin_recv,
    *, dims, cap,
):
    zs, xs, cs = dims
    ep_count = zs * xs * cs
    per = xs * cs
    chunk = per * cap
    rows, width = moe_in.shape
    col = width // 4
    half = col // 2
    conv_rows = conv_hbm.shape[0]
    conv_width = conv_hbm.shape[1]
    reach = taps_in.shape[0] - 1
    lead = 32
    span = conv_rows // 4
    tile = span // 2
    subs = 4
    sub = span // subs
    wide = width // 2

    me_ep, me = lax.axis_index("ep"), lax.axis_index("tp")
    core = lax.rem(me_ep, cs)
    mx = lax.rem(lax.div(me_ep, cs), xs)
    mz = lax.div(me_ep, cs * xs)
    nxt, prv = lax.rem(me + 1, 4), lax.rem(me + 3, 4)
    opp = lax.rem(me + 2, 4)

    def remote(src, dst, send, recv, where):
        return pltpu.make_async_remote_copy(
            src_ref=src, dst_ref=dst, send_sem=send, recv_sem=recv, device_id=where,
            device_id_type=MESH,
        )

    def aligned(start, size):
        return pl.ds(pl.multiple_of(start, size), size)

    def depth(c):
        t = lax.rem(c + 1, zs)
        sign = lax.rem(t, 2) * 2 - 1
        return sign * lax.div(t + 1, 2)

    def partner(c, j, way):
        dx, dc = j // cs, j % cs
        z = lax.rem(mz + way * depth(c) + zs, zs)
        x = lax.rem(mx + way * dx + xs, xs)
        return (z * xs + x) * cs + lax.rem(core + dc, cs)

    loads = [pltpu.make_async_copy(conv_hbm, padded.at[lead:], load_sem.at[0])]
    loads.append(pltpu.make_async_copy(proj_hbm, proj, load_sem.at[1]))
    for k in range(4):
        at = lax.rem(me + k, 4) * col
        loads.append(pltpu.make_async_copy(gate_hbm.at[0, aligned(at, col), :], gate.at[k], load_sem.at[2 + k]))
        loads.append(pltpu.make_async_copy(up_hbm.at[0, aligned(at, col), :], up.at[k], load_sem.at[6 + k]))
        loads.append(pltpu.make_async_copy(down_hbm.at[0, :, aligned(at, col)], down.at[k], load_sem.at[10 + k]))
    for load in loads:
        load.start()

    barrier = pltpu.get_barrier_semaphore()
    for k in range(1, 4):
        pl.semaphore_signal(barrier, inc=1, device_id={"tp": lax.rem(me + k, 4)}, device_id_type=MESH)

    def greet(d, carry):
        pl.semaphore_signal(
            barrier, inc=1, device_id={"ep": lax.rem(me_ep + d, ep_count)}, device_id_type=MESH
        )
        return carry

    lax.fori_loop(1, ep_count, greet, 0)

    value = moe_in[...].astype(f32)
    normed = (
        value * lax.rsqrt(jnp.mean(value * value, axis=1, keepdims=True) + 1e-06) * moe_gain[...]
    ).astype(bf16)
    for b in range(5):
        own[b] = normed[:, (b % 4) * col : (b % 4 + 1) * col]

    group_rows = routes.shape[1]
    s_at = lax.broadcasted_iota(i32, (ep_count, group_rows), 0)
    per_bits, core_bits = per.bit_length() - 1, cs.bit_length() - 1
    t = ((s_at >> per_bits) + 1) & (zs - 1)
    dz = ((t & 1) * 2 - 1) * ((t + 1) >> 1)
    dx = (s_at & (per - 1)) >> core_bits
    dc = s_at & (cs - 1)
    expert = ((((mz + dz + zs) & (zs - 1)) * xs + ((mx + dx) & (xs - 1))) * cs) + ((core + dc) & (cs - 1))
    first, second = routes[0:1, :] == expert, routes[1:2, :] == expert
    hit = first | second
    before = (
        lax.broadcasted_iota(i32, (group_rows, group_rows), 0)
        < lax.broadcasted_iota(i32, (group_rows, group_rows), 1)
    )
    rank = jnp.dot(
        jnp.where(hit, 1.0, 0.0).astype(bf16), jnp.where(before, 1.0, 0.0).astype(bf16),
        preferred_element_type=f32,
    )
    ranks[...] = jnp.where(hit, rank, -1.0)
    held_w[...] = jnp.where(first, weights[0:1, :], 0.0) + jnp.where(second, weights[1:2, :], 0.0)
    taps[0 : reach + 1, :] = taps_in[...].astype(f32)

    pl.semaphore_wait(barrier, ep_count + 2)

    a2a = []
    for k in range(1, 4):
        to = lax.rem(me + k, 4)
        a2a.append(
            remote(
                own.at[pl.ds(to, 2)], group.at[:, aligned(me * rows, rows), :],
                a2a_send.at[k - 1], a2a_recv.at[k - 1], {"tp": to},
            )
        )
    for r in a2a:
        r.start()
    group[:, aligned(me * rows, rows), :] = own[pl.ds(me, 2)]
    loads[0].wait()
    hist = remote(
        padded.at[lead + conv_rows - lead : lead + conv_rows], history, hist_send, hist_recv,
        {"ep": lax.rem(me_ep + 1, ep_count)},
    )
    hist.start()

    lane, strip = 128, 64

    def conv_tile(i, carry):
        for h in range(tile // strip):
            r0 = pl.multiple_of(i * tile + h * strip, strip)
            one = jnp.zeros((strip, lane), f32)
            two = jnp.zeros((strip, lane), f32)
            for n in range(0, conv_width, lane):
                x = padded[pl.ds(r0, strip + lead), n : n + lane].astype(f32)
                out = None
                for phase in range(8):
                    acc = None
                    extra = 8 if phase else 0
                    for q in range(lead // 8 + 1):
                        tap = 8 * q + phase - (lead - reach)
                        if tap < 0 or tap > reach:
                            continue
                        term = x[8 * q : 8 * q + strip + extra] * taps[tap : tap + 1, n : n + lane]
                        acc = term if acc is None else acc + term
                    if acc is None:
                        continue
                    part = acc[phase : phase + strip]
                    out = part if out is None else out + part
                mixed[pl.ds(r0, strip), n : n + lane] = out
                one = one + out
                two = two + out * out
            sums[0, h * strip : (h + 1) * strip, :] = one
            sums[1, h * strip : (h + 1) * strip, :] = two
        for m in range(2):
            stats[m, pl.ds(i, 1), :] = jnp.sum(sums[m].T, axis=0, keepdims=True)
        return carry

    tiles = conv_rows // tile
    lax.fori_loop(1, 4, conv_tile, 0)

    for r in a2a:
        r.wait_recv()

    slot = lax.broadcasted_iota(i32, (cap, group_rows), 0).astype(f32)

    def ep_copy(c, j):
        s = c * per + j
        return remote(
            outgoing.at[:, aligned(s * cap, cap), :],
            arrived.at[0:2, aligned(s * cap, cap), :],
            ep_send.at[s], ep_recv.at[s], {"ep": partner(c, j, 1)},
        )

    def dispatch(c, carry):
        ranked = ranks[aligned(c * per, per), :]
        pick = jnp.concatenate(
            [jnp.where(ranked[j : j + 1, :] == slot, 1.0, 0.0) for j in range(per)], axis=0
        ).astype(bf16)
        here = aligned(c * chunk, chunk)
        for b in range(2):
            outgoing[b, here, :] = jnp.dot(pick, group[b], preferred_element_type=f32).astype(bf16)

        for j in range(per):
            if j == 0:
                @pl.when(c < zs - 1)
                def _():
                    ep_copy(c, 0).start()
            else:
                ep_copy(c, j).start()
        return carry

    lax.fori_loop(0, zs, dispatch, 0)
    mine = slice((zs - 1) * chunk, (zs - 1) * chunk + cap)
    arrived[0:2, mine, :] = outgoing[:, mine, :]

    lax.fori_loop(4, tiles, conv_tile, 0)
    hist.wait_recv()
    padded[0:lead, :] = jnp.where(me_ep == 0, jnp.zeros((lead, conv_width), bf16), history[...])
    lax.fori_loop(0, 1, conv_tile, 0)

    moments = [
        remote(stats, stats_in.at[k - 1], stat_send.at[k - 1], stat_recv.at[k - 1], {"tp": lax.rem(me + k, 4)})
        for k in range(1, 4)
    ]
    for r in moments:
        r.start()

    def weigh(c, carry):
        ranked = ranks[aligned(c * per, per), :]
        held = held_w[aligned(c * per, per), :]
        block = jnp.concatenate(
            [jnp.where(ranked[j : j + 1, :] == slot, held[j : j + 1, :], 0.0) for j in range(per)], axis=0
        )
        scale[c] = block.T.astype(bf16)
        return carry

    lax.fori_loop(0, zs, weigh, 0)

    def center_and_scale():
        for r in moments:
            r.wait_recv()
        total = (stats[...] + stats_in[0] + stats_in[1] + stats_in[2]) / width
        center = total[0]
        spread = jnp.maximum(total[1] - center * center, 0.0)
        inverse = lax.rsqrt(spread + 1e-05)
        for i in range(tiles):
            both = jnp.concatenate([center[i : i + 1], inverse[i : i + 1]] + [center[i : i + 1]] * 6, axis=0)
            columns[i * tile : (i + 1) * tile, :] = both.T

    step_cols = min(512, width)

    def project(k, h):
        at = lax.rem(me + k, 4) * span + h * tile
        view = aligned(at, tile)
        stat = columns[view, :]
        scaled = (mixed[view, :] - stat[:, 0:1]) * stat[:, 1:2] * gain[...] + shift[...]
        activated = (scaled / (1.0 + jnp.exp(-scaled))).astype(bf16)
        for n in range(0, width, step_cols):
            partial[k, aligned(h * tile, tile), n : n + step_cols] = jnp.dot(
                activated, proj[:, n : n + step_cols], preferred_element_type=f32
            ).astype(bf16)

    def conv_copies(j):
        at = aligned(j * sub, sub)
        low, high = slice(0, wide), slice(wide, width)

        def one(n, src, dst, where):
            return remote(src, dst, conv_send.at[n, j], conv_recv.at[n, j], {"tp": where})

        return [
            one(0, partial.at[2, at, low], conv_a.at[at, :], nxt),
            one(1, partial.at[2, at, high], conv_b.at[at, :], prv),
            one(2, partial.at[1, at, high], conv_c.at[at, high], nxt),
            one(3, partial.at[3, at, low], conv_d.at[at, low], prv),
            one(4, conv_u.at[at, :], conv_c.at[at, low], nxt),
            one(5, conv_v.at[at, :], conv_d.at[at, high], prv),
        ]

    def conv_first(j):
        for r in conv_copies(j)[:4]:
            r.start()

    def conv_second(j):
        copies = conv_copies(j)
        at = aligned(j * sub, sub)
        copies[0].wait_recv()
        conv_u[at, :] = (partial[1, at, :wide].astype(f32) + conv_a[at, :].astype(f32)).astype(bf16)
        copies[4].start()
        copies[1].wait_recv()
        conv_v[at, :] = (partial[3, at, wide:].astype(f32) + conv_b[at, :].astype(f32)).astype(bf16)
        copies[5].start()

    def conv_last(j, carry):
        copies = conv_copies(j)
        at = aligned(j * sub, sub)
        for n in (2, 3, 4, 5):
            copies[n].wait_recv()
        conv_out[at, :] = (
            partial[0, at, :].astype(f32) + conv_c[at, :].astype(f32) + conv_d[at, :].astype(f32)
        ).astype(bf16)
        return carry

    def gather_copies(c):
        at = aligned(c * chunk, chunk)
        return [
            remote(arrived.at[1, at, :], arrived.at[2, at, :], gather_send.at[0, c], gather_recv.at[0, c], {"tp": prv}),
            remote(arrived.at[0, at, :], arrived.at[3, at, :], gather_send.at[1, c], gather_recv.at[1, c], {"tp": nxt}),
        ]

    def land(c):
        for j in range(per):
            if j == 0:
                @pl.when(c < zs - 1)
                def _():
                    ep_copy(c, 0).wait_recv()
            else:
                ep_copy(c, j).wait_recv()
        for r in gather_copies(c):
            r.start()

    def return_copies(c):
        at = aligned(c * chunk, chunk)
        low, high = slice(0, half), slice(half, col)

        def one(n, src, dst, where):
            return remote(src, dst, ret_send.at[n, c], ret_recv.at[n, c], {"tp": where})

        return [
            one(0, pieces.at[2, at, low], moe_a.at[at, :], nxt),
            one(1, pieces.at[2, at, high], moe_b.at[at, :], prv),
            one(2, pieces.at[1, at, high], moe_c.at[at, high], nxt),
            one(3, pieces.at[3, at, low], moe_d.at[at, low], prv),
            one(4, moe_u.at[at, :], moe_c.at[at, low], nxt),
            one(5, moe_v.at[at, :], moe_d.at[at, high], prv),
        ]

    def experts(c):
        for r in gather_copies(c):
            r.wait_recv()
        at = aligned(c * chunk, chunk)
        lines = [arrived[k, at, :] for k in range(4)]
        hidden = []
        step = min(256, col)
        for n in range(0, col, step):
            left = sum(jnp.dot(lines[k], gate[k, :, n : n + step], preferred_element_type=f32) for k in range(4))
            right = sum(jnp.dot(lines[k], up[k, :, n : n + step], preferred_element_type=f32) for k in range(4))
            hidden.append((left / (1.0 + jnp.exp(-left)) * right).astype(bf16))
        hid = jnp.concatenate(hidden, axis=1)
        for k in (2, 1, 3, 0):
            pieces[k, at, :] = jnp.dot(hid, down[k], preferred_element_type=f32).astype(bf16)
        for r in return_copies(c)[:4]:
            r.start()

    def middle(c):
        copies = return_copies(c)
        at = aligned(c * chunk, chunk)
        copies[0].wait_recv()
        moe_u[at, :] = (pieces[1, at, :half].astype(f32) + moe_a[at, :].astype(f32)).astype(bf16)
        copies[4].start()
        copies[1].wait_recv()
        moe_v[at, :] = (pieces[3, at, half:].astype(f32) + moe_b[at, :].astype(f32)).astype(bf16)
        copies[5].start()

    def back_copy(c, j):
        s = c * per + j
        at = aligned(s * cap, cap)
        return remote(
            back_out.at[at, :], returned.at[at, :], back_send.at[s], back_recv.at[s],
            {"ep": partner(c, j, -1)},
        )

    def finish(c):
        copies = return_copies(c)
        at = aligned(c * chunk, chunk)
        for n in (2, 3, 4, 5):
            copies[n].wait_recv()
        back_out[at, :] = (
            pieces[0, at, :].astype(f32) + moe_c[at, :].astype(f32) + moe_d[at, :].astype(f32)
        ).astype(bf16)
        for j in range(per):
            if j == 0:
                @pl.when(c < zs - 1)
                def _():
                    back_copy(c, 0).start()
            else:
                back_copy(c, j).start()

    def step(i, carry):
        @pl.when(i < zs)
        def _():
            land(i)

        @pl.when(i == 0)
        def _():
            center_and_scale()
            loads[1].wait()

        @pl.when(i < 2)
        def _():
            def both(h, inner):
                project(2 + i, h)
                project(1 - i, h)
                return inner

            lax.fori_loop(0, 2, both, 0)

        @pl.when((i >= 2) & (i < 2 + subs))
        def _():
            conv_first(i - 2)

        @pl.when((i >= 1) & (i <= zs))
        def _():
            middle(i - 1)

        @pl.when((i >= 3) & (i < 3 + subs))
        def _():
            conv_second(i - 3)

        @pl.when((i >= 2) & (i < zs + 2))
        def _():
            finish(i - 2)

        @pl.when(i == 0)
        def _():
            for load in loads[2:]:
                load.wait()

        @pl.when(i < zs)
        def _():
            experts(i)

        return carry

    lax.fori_loop(0, max(zs + 2, subs + 3), step, 0)
    lax.fori_loop(0, subs, conv_last, 0)

    returned[mine, :] = back_out[mine, :]
    total = jnp.zeros((group_rows, col), f32)
    for c in range(zs):
        for j in range(per):
            if (c, j) != (zs - 1, 0):
                back_copy(c, j).wait_recv()
        total = total + jnp.dot(
            scale[c], returned[c * chunk : (c + 1) * chunk, :], preferred_element_type=f32
        )
    combined[...] = total.astype(bf16)
    last = []
    for k in range(1, 4):
        to = lax.rem(me + k, 4)
        last.append(
            remote(
                combined.at[aligned(to * rows, rows), :], final.at[me],
                fin_send.at[k - 1], fin_recv.at[k - 1], {"tp": to},
            )
        )
    for r in last:
        r.start()
    final[me] = combined[aligned(me * rows, rows), :]
    for r in last:
        r.wait_recv()
    for b in range(4):
        moe_out[:, b * col : (b + 1) * col] = final[b]

    for r in a2a + [hist] + moments + last:
        r.wait_send()

    def drain(c, carry):
        for j in range(per):
            if j == 0:
                @pl.when(c < zs - 1)
                def _():
                    ep_copy(c, 0).wait_send()
                    back_copy(c, 0).wait_send()
            else:
                ep_copy(c, j).wait_send()
                back_copy(c, j).wait_send()
        for r in gather_copies(c) + return_copies(c):
            r.wait_send()
        return carry

    lax.fori_loop(0, zs, drain, 0)

    def conv_drain(j, carry):
        for r in conv_copies(j):
            r.wait_send()
        return carry

    lax.fori_loop(0, subs, conv_drain, 0)


def local(
    conv_input, conv_kernel, norm_gain, norm_shift, conv_proj, moe_input, moe_gain,
    routes, route_weights, gate_proj, up_proj, down_proj, *, dims=DIMS,
):
    zs, xs, cs = dims
    ep_count = zs * xs * cs
    conv_rows, conv_width = conv_input.shape
    rows, width = moe_input.shape
    group_rows = routes.shape[0]
    cap = 16
    slots = ep_count * cap
    col, half, wide = width // 4, width // 8, width // 2
    span = conv_rows // 4
    tile = span // 2
    tiles = conv_rows // tile
    hid = gate_proj.shape[2]
    chunk = xs * cs * cap
    reach = conv_kernel.shape[0] - 1
    vmem, dma = pltpu.VMEM, pltpu.SemaphoreType.DMA
    at_vmem, at_any = pl.BlockSpec(memory_space=pltpu.VMEM), pl.BlockSpec(memory_space=pl.ANY)
    scratch = [
        vmem((32 + conv_rows, conv_width), bf16),
        vmem((32, conv_width), f32),
        vmem((conv_rows, conv_width), f32),
        vmem((2, tile, 128), f32),
        vmem((2, tiles, tile), f32),
        vmem((3, 2, tiles, tile), f32),
        vmem((conv_rows, 8), f32),
        vmem((conv_width, width), bf16),
        vmem((4, span, width), bf16),
        vmem((span, wide), bf16), vmem((span, wide), bf16),
        vmem((span, width), bf16), vmem((span, width), bf16),
        vmem((span, wide), bf16), vmem((span, wide), bf16),
        vmem((32, conv_width), bf16),
        vmem((4, col, hid), bf16), vmem((4, col, hid), bf16), vmem((4, hid, col), bf16),
        vmem((5, rows, col), bf16),
        vmem((2, group_rows, col), bf16),
        vmem((ep_count, group_rows), f32), vmem((ep_count, group_rows), f32),
        vmem((zs, group_rows, chunk), bf16),
        vmem((2, slots, col), bf16),
        vmem((4, slots, col), bf16),
        vmem((4, slots, col), bf16),
        vmem((slots, half), bf16), vmem((slots, half), bf16),
        vmem((slots, col), bf16), vmem((slots, col), bf16),
        vmem((slots, half), bf16), vmem((slots, half), bf16),
        vmem((slots, col), bf16), vmem((slots, col), bf16),
        vmem((group_rows, col), bf16),
        vmem((4, rows, col), bf16),
        dma((14,)),
        dma, dma,
        dma((3,)), dma((3,)),
        dma((3,)), dma((3,)),
        dma((ep_count,)), dma((ep_count,)),
        dma((2, zs)), dma((2, zs)),
        dma((6, zs)), dma((6, zs)),
        dma((ep_count,)), dma((ep_count,)),
        dma((6, 4)), dma((6, 4)),
        dma((3,)), dma((3,)),
    ]
    return pl.pallas_call(
        functools.partial(layer, dims=dims, cap=cap),
        out_shape=(
            jax.ShapeDtypeStruct((span, width), bf16),
            jax.ShapeDtypeStruct((rows, width), bf16),
        ),
        in_specs=[at_vmem] * 7 + [at_any] * 5,
        out_specs=(at_vmem, at_vmem),
        scratch_shapes=scratch,
        compiler_params=pltpu.CompilerParams(
            collective_id=0, has_side_effects=True, vmem_limit_bytes=60 * 1024 * 1024
        ),
    )(
        moe_input, moe_gain[None, :], routes.T, route_weights.T, conv_kernel, norm_gain[None, :],
        norm_shift[None, :], conv_input, conv_proj, gate_proj, up_proj, down_proj,
    )


def solution(mesh):
    placed = (
        P("ep", "tp"),
        P(None, "tp"),
        P("tp"),
        P("tp"),
        P("tp", None),
        P(("ep", "tp"), None),
        P(),
        P("ep", None),
        P("ep", None),
        P("ep", None, "tp"),
        P("ep", None, "tp"),
        P("ep", "tp", None),
    )
    return jax.shard_map(
        local,
        mesh=mesh,
        in_specs=placed,
        out_specs=(P(("ep", "tp"), None), P(("ep", "tp"), None)),
        check_vma=False,
    )
```

```python
import functools

import jax
import jax.numpy as jnp
from jax import lax
from jax.experimental import pallas as pl
from jax.experimental.pallas import tpu as pltpu
from jax.sharding import PartitionSpec as P

MESH = pl.DeviceIdType.MESH
DIMS = (8, 4, 2)
f32, bf16, i32 = jnp.float32, jnp.bfloat16, jnp.int32


def layer(
    moe_in, moe_gain, routes, weights, taps_in, gain, shift, conv_hbm, proj_hbm, gate_hbm, up_hbm, down_hbm,
    conv_out, moe_out,
    padded, xin, history, taps_src, taps_all, taps, affine_src, affine, mixed, sums, act, wfull, conv_v,
    gate, up, down, own, group, ranks, held_w, scale, outgoing, arrived, pieces,
    moe_a, moe_b, moe_c, moe_d, moe_u, moe_v, back_out, returned, combined, final,
    load_sem, out_sem, ready, hist_send, hist_recv, relay_send, relay_recv, a2a_send, a2a_recv,
    cx_send, cx_recv, tap_send, tap_recv, aff_send, aff_recv,
    wy_send, wy_recv, wx_send, wx_recv, wd_send, wd_recv, ep_send, ep_recv,
    gather_send, gather_recv, ret_send, ret_recv, back_send, back_recv, fin_send, fin_recv,
    *, dims, cap,
):
    zs, xs, cs = dims
    ep_count = zs * xs * cs
    per = xs * cs
    chunk = per * cap
    rows, width = moe_in.shape
    col = width // 4
    half = col // 2
    conv_rows = conv_hbm.shape[0]
    conv_width = conv_hbm.shape[1]
    reach = taps_in.shape[0] - 1
    lead = 32
    span = conv_rows // 4
    slice_cols = width // per

    me_ep, me = lax.axis_index("ep"), lax.axis_index("tp")
    core = lax.rem(me_ep, cs)
    mx = lax.rem(lax.div(me_ep, cs), xs)
    mz = lax.div(me_ep, cs * xs)
    nxt, prv = lax.rem(me + 1, 4), lax.rem(me + 3, 4)

    def remote(src, dst, send, recv, where):
        return pltpu.make_async_remote_copy(
            src_ref=src, dst_ref=dst, send_sem=send, recv_sem=recv, device_id=where,
            device_id_type=MESH,
        )

    def aligned(start, size):
        return pl.ds(pl.multiple_of(start, size), size)

    def depth(c):
        t = c + lax.div(c + zs - 2, zs - 1) - (zs - 1) * lax.div(c, zs - 1)
        sign = lax.rem(t, 2) * 2 - 1
        return sign * lax.div(t + 1, 2)

    def place(z, x, c):
        return (z * xs + x) * cs + c

    def partner(c, j, way):
        dx, dc = j // cs, j % cs
        z = lax.rem(mz + way * depth(c) + zs, zs)
        x = lax.rem(mx + way * dx + xs, xs)
        return place(z, x, lax.rem(core + dc, cs))

    barrier = pltpu.get_barrier_semaphore()
    along_z = sorted(range(1, zs), key=lambda d: -min(d, zs - d))
    for d in along_z:
        pl.semaphore_signal(
            barrier, inc=1, device_id={"ep": place(lax.rem(mz + d, zs), mx, core)}, device_id_type=MESH
        )
    for k in (2, 1, 3):
        pl.semaphore_signal(barrier, inc=1, device_id={"tp": lax.rem(me + k, 4)}, device_id_type=MESH)
    for j in range(1, per):
        where = place(mz, lax.rem(mx + j // cs, xs), lax.rem(core + j % cs, cs))
        pl.semaphore_signal(barrier, inc=1, device_id={"ep": where}, device_id_type=MESH)

    loads = [pltpu.make_async_copy(conv_hbm, padded.at[lead:], load_sem.at[0])]
    proj_loads = [
        pltpu.make_async_copy(
            proj_hbm.at[:, q * slice_cols : (q + 1) * slice_cols], wfull.at[q, me], load_sem.at[13 + q]
        )
        for q in range(per)
    ]
    for k in range(4):
        at = lax.rem(me + k, 4) * col
        loads.append(pltpu.make_async_copy(gate_hbm.at[0, aligned(at, col), :], gate.at[k], load_sem.at[1 + k]))
        loads.append(pltpu.make_async_copy(up_hbm.at[0, aligned(at, col), :], up.at[k], load_sem.at[5 + k]))
        loads.append(pltpu.make_async_copy(down_hbm.at[0, :, aligned(at, col)], down.at[k], load_sem.at[9 + k]))
    for load in loads[:1] + proj_loads + loads[1:]:
        load.start()

    value = moe_in[...].astype(f32)
    normed = (
        value * lax.rsqrt(jnp.mean(value * value, axis=1, keepdims=True) + 1e-06) * moe_gain[...]
    ).astype(bf16)
    for b in range(5):
        own[b] = normed[:, (b % 4) * col : (b % 4 + 1) * col]

    group_rows = routes.shape[1]
    s_at = lax.broadcasted_iota(i32, (ep_count, group_rows), 0)
    per_bits, core_bits = per.bit_length() - 1, cs.bit_length() - 1
    c_at = s_at >> per_bits
    t = jnp.where(c_at == 0, 0, jnp.where(c_at == zs - 1, 1, c_at + 1))
    dz = ((t & 1) * 2 - 1) * ((t + 1) >> 1)
    dx = (s_at & (per - 1)) >> core_bits
    dc = s_at & (cs - 1)
    expert = ((((mz + dz + zs) & (zs - 1)) * xs + ((mx + dx) & (xs - 1))) * cs) + ((core + dc) & (cs - 1))
    first, second = routes[0:1, :] == expert, routes[1:2, :] == expert
    hit = first | second
    before = (
        lax.broadcasted_iota(i32, (group_rows, group_rows), 0)
        < lax.broadcasted_iota(i32, (group_rows, group_rows), 1)
    )
    rank = jnp.dot(
        jnp.where(hit, 1.0, 0.0).astype(bf16), jnp.where(before, 1.0, 0.0).astype(bf16),
        preferred_element_type=f32,
    )
    ranks[...] = jnp.where(hit, rank, -1.0)
    held_w[...] = jnp.where(first, weights[0:1, :], 0.0) + jnp.where(second, weights[1:2, :], 0.0)
    taps_src[...] = jnp.zeros_like(taps_src)
    taps_src[0 : reach + 1, :] = taps_in[...]
    affine_src[0:1, :] = gain[...]
    affine_src[1:2, :] = shift[...]
    padded[0:lead, :] = jnp.zeros((lead, conv_width), bf16)
    sums[...] = jnp.zeros_like(sums)

    pl.semaphore_wait(barrier, zs + per + 1)

    a2a, conv_x, params = [], [], []
    for k in range(1, 4):
        to = lax.rem(me + k, 4)
        a2a.append(
            remote(
                own.at[pl.ds(to, 2)], group.at[:, aligned(me * rows, rows), :],
                a2a_send.at[k - 1], a2a_recv.at[k - 1], {"tp": to},
            )
        )
        conv_x.append(
            remote(
                padded.at[pl.ds(pl.multiple_of(to * span, span), span + lead), :], xin.at[me],
                cx_send.at[k - 1], cx_recv.at[k - 1], {"tp": to},
            )
        )
        params.append(remote(taps_src, taps_all.at[me], tap_send.at[k - 1], tap_recv.at[k - 1], {"tp": to}))
        params.append(remote(affine_src, affine.at[me], aff_send.at[k - 1], aff_recv.at[k - 1], {"tp": to}))
    for r in a2a:
        r.start()
    for d in along_z:
        pl.semaphore_signal(
            ready, inc=1, device_id={"ep": place(lax.rem(mz + d, zs), mx, core)}, device_id_type=MESH
        )
    loads[0].wait()
    group[:, aligned(me * rows, rows), :] = own[pl.ds(me, 2)]
    xin[me] = padded[pl.ds(pl.multiple_of(me * span, span), span + lead), :]
    taps_all[me] = taps_src[...]
    affine[me] = affine_src[...]

    hist = remote(
        padded.at[conv_rows : conv_rows + lead], history.at[4], hist_send, hist_recv,
        {"ep": lax.rem(me_ep + 1, ep_count)},
    )

    def hist_relay(k):
        return remote(history.at[4], history.at[k], relay_send.at[k - 1], relay_recv.at[k - 1], {"tp": 0 * me})

    def pass_history():
        hist.wait_recv()
        for k in range(1, 4):
            @pl.when(me == k)
            def _():
                hist_relay(k).start()

    pl.semaphore_wait(ready, zs - 1)
    hist.start()

    lane, strip = 128, min(64, span)
    strips = span // strip

    def conv_block(b):
        def conv_strip(i, carry):
            at = aligned(i * strip, strip)
            r0 = pl.multiple_of(i * strip, strip)
            one = jnp.zeros((strip, lane), f32)
            two = jnp.zeros((strip, lane), f32)
            for n in range(0, conv_width, lane):
                x = xin[b, pl.ds(r0, strip + lead), n : n + lane].astype(f32)
                out = None
                for phase in range(8):
                    acc = None
                    extra = 8 if phase else 0
                    for q in range(lead // 8 + 1):
                        tap = 8 * q + phase - (lead - reach)
                        if tap < 0 or tap > reach:
                            continue
                        term = x[8 * q : 8 * q + strip + extra] * taps[b, tap : tap + 1, n : n + lane]
                        acc = term if acc is None else acc + term
                    if acc is None:
                        continue
                    part = acc[phase : phase + strip]
                    out = part if out is None else out + part
                mixed[b, at, n : n + lane] = out
                one = one + out
                two = two + out * out
            sums[0, at, :] = sums[0, at, :] + one
            sums[1, at, :] = sums[1, at, :] + two
            return carry

        lax.fori_loop(0, strips, conv_strip, 0)

    def normalise(i, carry):
        at = aligned(i * strip, strip)
        center = jnp.sum(sums[0, at, :], axis=1, keepdims=True) / width
        square = jnp.sum(sums[1, at, :], axis=1, keepdims=True) / width
        inverse = lax.rsqrt(jnp.maximum(square - center * center, 0.0) + 1e-05)
        for b in range(4):
            scaled = (mixed[b, at, :] - center) * inverse * affine[b, 0:1, :] + affine[b, 1:2, :]
            act[b, at, :] = (scaled / (1.0 + jnp.exp(-scaled))).astype(bf16)
        return carry

    def take_history(k):
        @pl.when(me == 0)
        def _():
            b = (4 - k) % 4
            if b:
                hist_relay(b).wait_recv()
            before_rows = history[4 if b == 0 else b]
            xin[b, 0:lead, :] = jnp.where(me_ep == 0, jnp.zeros_like(before_rows), before_rows)

    def convolve(k):
        b = lax.rem(me + 4 - k, 4)
        if k:
            params[2 * k - 2].wait_recv()
            params[2 * k - 1].wait_recv()
            conv_x[k - 1].wait_recv()
        taps[b] = taps_all[b].astype(f32)
        take_history(k)
        conv_block(b)

    slice_id = mx * cs + core

    def w_first(k):
        piece = wfull.at[slice_id, me]
        return remote(piece, piece, wy_send.at[k - 1], wy_recv.at[k - 1], {"tp": lax.rem(me + k, 4)})

    def w_along(k, d):
        piece = wfull.at[slice_id, lax.rem(me + 4 - k, 4)]
        return remote(
            piece, piece, wx_send.at[d - 1, k - 1], wx_recv.at[d - 1, k - 1],
            {"ep": place(mz, lax.rem(mx + d, xs), core)},
        )

    def w_across(k, d):
        piece = wfull.at[lax.rem(mx + xs - d, xs) * cs + core, lax.rem(me + 4 - k, 4)]
        return remote(
            piece, piece, wd_send.at[d, k - 1], wd_recv.at[d, k - 1],
            {"ep": place(mz, mx, lax.rem(core + 1, cs))},
        )

    def w_spread(k):
        w_first(k).wait_recv()
        for d in range(1, xs):
            w_along(k, d).start()
        if cs > 1:
            w_across(k, 0).start()

    def w_share(k):
        for d in range(1, xs):
            w_along(k, d).wait_recv()
            if cs > 1:
                w_across(k, d).start()

    def multiply(side):
        def one(d, carry):
            q = lax.rem(mx + d, xs) * cs + lax.rem(core + side, cs)
            total = sum(jnp.dot(act[b], wfull[q, b], preferred_element_type=f32) for b in range(4))
            conv_v[:, aligned(q * slice_cols, slice_cols)] = total.astype(bf16)
            return carry

        lax.fori_loop(0, xs, one, 0)

    for r in a2a:
        r.wait_recv()
    pass_history()
    for r in params + conv_x:
        r.start()

    slot = lax.broadcasted_iota(i32, (cap, group_rows), 0).astype(f32)

    def ep_copy(c, j):
        s = c * per + j
        return remote(
            outgoing.at[:, aligned(s * cap, cap), :],
            arrived.at[0:2, aligned(s * cap, cap), :],
            ep_send.at[s], ep_recv.at[s], {"ep": partner(c, j, 1)},
        )

    def dispatch(c, carry):
        ranked = ranks[aligned(c * per, per), :]
        pick = jnp.concatenate(
            [jnp.where(ranked[j : j + 1, :] == slot, 1.0, 0.0) for j in range(per)], axis=0
        ).astype(bf16)
        here = aligned(c * chunk, chunk)
        for b in range(2):
            outgoing[b, here, :] = jnp.dot(pick, group[b], preferred_element_type=f32).astype(bf16)

        for j in range(per):
            if j == 0:
                @pl.when(c > 0)
                def _():
                    ep_copy(c, 0).start()
            else:
                ep_copy(c, j).start()
        return carry

    lax.fori_loop(0, zs, dispatch, 0)
    mine = slice(0, cap)
    arrived[0:2, mine, :] = outgoing[:, mine, :]

    def weigh(c, carry):
        ranked = ranks[aligned(c * per, per), :]
        held = held_w[aligned(c * per, per), :]
        block = jnp.concatenate(
            [jnp.where(ranked[j : j + 1, :] == slot, held[j : j + 1, :], 0.0) for j in range(per)], axis=0
        )
        scale[c] = block.T.astype(bf16)
        return carry

    lax.fori_loop(0, zs, weigh, 0)

    def gather_copies(c):
        at = aligned(c * chunk, chunk)
        return [
            remote(arrived.at[1, at, :], arrived.at[2, at, :], gather_send.at[0, c], gather_recv.at[0, c], {"tp": prv}),
            remote(arrived.at[0, at, :], arrived.at[3, at, :], gather_send.at[1, c], gather_recv.at[1, c], {"tp": nxt}),
        ]

    def land(c):
        for j in range(per):
            if j == 0:
                @pl.when(c > 0)
                def _():
                    ep_copy(c, 0).wait_recv()
            else:
                ep_copy(c, j).wait_recv()
        for r in gather_copies(c):
            r.start()

    def return_copies(c):
        at = aligned(c * chunk, chunk)
        low, high = slice(0, half), slice(half, col)

        def one(n, src, dst, where):
            return remote(src, dst, ret_send.at[n, c], ret_recv.at[n, c], {"tp": where})

        return [
            one(0, pieces.at[2, at, low], moe_a.at[at, :], nxt),
            one(1, pieces.at[2, at, high], moe_b.at[at, :], prv),
            one(2, pieces.at[1, at, high], moe_c.at[at, high], nxt),
            one(3, pieces.at[3, at, low], moe_d.at[at, low], prv),
            one(4, moe_u.at[at, :], moe_c.at[at, low], nxt),
            one(5, moe_v.at[at, :], moe_d.at[at, high], prv),
        ]

    def experts(c):
        for r in gather_copies(c):
            r.wait_recv()
        at = aligned(c * chunk, chunk)
        lines = [arrived[k, at, :] for k in range(4)]
        hidden = []
        step = min(256, col)
        for n in range(0, col, step):
            left = sum(jnp.dot(lines[k], gate[k, :, n : n + step], preferred_element_type=f32) for k in range(4))
            right = sum(jnp.dot(lines[k], up[k, :, n : n + step], preferred_element_type=f32) for k in range(4))
            hidden.append((left / (1.0 + jnp.exp(-left)) * right).astype(bf16))
        hid = jnp.concatenate(hidden, axis=1)
        for k in (2, 1, 3, 0):
            pieces[k, at, :] = jnp.dot(hid, down[k], preferred_element_type=f32).astype(bf16)
        for r in return_copies(c)[:4]:
            r.start()

    def middle(c):
        copies = return_copies(c)
        at = aligned(c * chunk, chunk)
        copies[0].wait_recv()
        moe_u[at, :] = (pieces[1, at, :half].astype(f32) + moe_a[at, :].astype(f32)).astype(bf16)
        copies[4].start()
        copies[1].wait_recv()
        moe_v[at, :] = (pieces[3, at, half:].astype(f32) + moe_b[at, :].astype(f32)).astype(bf16)
        copies[5].start()

    def back_copy(c, j):
        s = c * per + j
        at = aligned(s * cap, cap)
        return remote(
            back_out.at[at, :], returned.at[at, :], back_send.at[s], back_recv.at[s],
            {"ep": partner(c, j, -1)},
        )

    def finish(c):
        copies = return_copies(c)
        at = aligned(c * chunk, chunk)
        for n in (2, 3, 4, 5):
            copies[n].wait_recv()
        back_out[at, :] = (
            pieces[0, at, :].astype(f32) + moe_c[at, :].astype(f32) + moe_d[at, :].astype(f32)
        ).astype(bf16)
        for j in range(per):
            if j == 0:
                @pl.when(c > 0)
                def _():
                    back_copy(c, 0).start()
            else:
                back_copy(c, j).start()

    land(0)

    def step(i, carry):
        @pl.when(i < zs - 1)
        def _():
            land(i + 1)

        @pl.when(i == 0)
        def _():
            for load in proj_loads:
                load.wait()
            w_first(1).start()
            w_first(3).start()
            for k in (0, 1, 3):
                convolve(k)
            for load in loads[1:]:
                load.wait()

        @pl.when(i == 1)
        def _():
            w_first(2).start()
            convolve(2)
            lax.fori_loop(0, strips, normalise, 0)

        for n, k in enumerate((1, 3, 2)):
            @pl.when(i == 2 + n)
            def _():
                w_spread(k)

            @pl.when(i == 5 + n)
            def _():
                w_share(k)

        @pl.when(i < zs)
        def _():
            experts(i)

        @pl.when(i == last_step - 1)
        def _():
            multiply(0)

        @pl.when((i >= 1) & (i <= zs))
        def _():
            middle(i - 1)

        @pl.when((i >= 2) & (i < zs + 2))
        def _():
            finish(i - 2)

        return carry

    last_step = max(zs + 1, 9)
    lax.fori_loop(0, last_step, step, 0)
    if cs > 1:
        for k in (1, 3, 2):
            for d in range(xs):
                w_across(k, d).wait_recv()
        multiply(1)
    put = pltpu.make_async_copy(conv_v, conv_out, out_sem)
    put.start()
    if last_step < zs + 2:
        finish(zs - 1)

    returned[mine, :] = back_out[mine, :]
    total = jnp.zeros((group_rows, col), f32)
    for c in range(zs):
        for j in range(per):
            if (c, j) != (0, 0):
                back_copy(c, j).wait_recv()
        total = total + jnp.dot(
            scale[c], returned[c * chunk : (c + 1) * chunk, :], preferred_element_type=f32
        )
    combined[...] = total.astype(bf16)
    last = []
    for k in range(1, 4):
        to = lax.rem(me + k, 4)
        last.append(
            remote(
                combined.at[aligned(to * rows, rows), :], final.at[me],
                fin_send.at[k - 1], fin_recv.at[k - 1], {"tp": to},
            )
        )
    for r in last:
        r.start()
    final[me] = combined[aligned(me * rows, rows), :]
    for r in last:
        r.wait_recv()
    for b in range(4):
        moe_out[:, b * col : (b + 1) * col] = final[b]

    for r in a2a + conv_x + params + [hist] + last:
        r.wait_send()
    for k in range(1, 4):
        w_first(k).wait_send()
        for d in range(1, xs):
            w_along(k, d).wait_send()
        if cs > 1:
            for d in range(xs):
                w_across(k, d).wait_send()

        @pl.when(me == k)
        def _():
            hist_relay(k).wait_send()

    def drain(c, carry):
        for j in range(per):
            if j == 0:
                @pl.when(c > 0)
                def _():
                    ep_copy(c, 0).wait_send()
                    back_copy(c, 0).wait_send()
            else:
                ep_copy(c, j).wait_send()
                back_copy(c, j).wait_send()
        for r in gather_copies(c) + return_copies(c):
            r.wait_send()
        return carry

    lax.fori_loop(0, zs, drain, 0)

    put.wait()


def local(
    conv_input, conv_kernel, norm_gain, norm_shift, conv_proj, moe_input, moe_gain,
    routes, route_weights, gate_proj, up_proj, down_proj, *, dims=DIMS,
):
    zs, xs, cs = dims
    ep_count = zs * xs * cs
    conv_rows, conv_width = conv_input.shape
    rows, width = moe_input.shape
    group_rows = routes.shape[0]
    cap = 16
    slots = ep_count * cap
    col, half = width // 4, width // 8
    span = conv_rows // 4
    hid = gate_proj.shape[2]
    chunk = xs * cs * cap
    per = xs * cs
    vmem, dma = pltpu.VMEM, pltpu.SemaphoreType.DMA
    at_vmem, at_any = pl.BlockSpec(memory_space=pltpu.VMEM), pl.BlockSpec(memory_space=pl.ANY)
    scratch = [
        vmem((32 + conv_rows, conv_width), bf16),
        vmem((4, 32 + span, conv_width), bf16),
        vmem((5, 32, conv_width), bf16),
        vmem((32, conv_width), bf16),
        vmem((4, 32, conv_width), bf16),
        vmem((4, 32, conv_width), f32),
        vmem((2, conv_width), f32),
        vmem((4, 2, conv_width), f32),
        vmem((4, span, conv_width), f32),
        vmem((2, span, 128), f32),
        vmem((4, span, conv_width), bf16),
        vmem((per, 4, conv_width, width // per), bf16),
        vmem((span, width), bf16),
        vmem((4, col, hid), bf16), vmem((4, col, hid), bf16), vmem((4, hid, col), bf16),
        vmem((5, rows, col), bf16),
        vmem((2, group_rows, col), bf16),
        vmem((ep_count, group_rows), f32), vmem((ep_count, group_rows), f32),
        vmem((zs, group_rows, chunk), bf16),
        vmem((2, slots, col), bf16),
        vmem((4, slots, col), bf16),
        vmem((4, slots, col), bf16),
        vmem((slots, half), bf16), vmem((slots, half), bf16),
        vmem((slots, col), bf16), vmem((slots, col), bf16),
        vmem((slots, half), bf16), vmem((slots, half), bf16),
        vmem((slots, col), bf16), vmem((slots, col), bf16),
        vmem((group_rows, col), bf16),
        vmem((4, rows, col), bf16),
        dma((13 + per,)), dma, pltpu.SemaphoreType.REGULAR,
        dma, dma,
        dma((3,)), dma((3,)),
        dma((3,)), dma((3,)),
        dma((3,)), dma((3,)),
        dma((3,)), dma((3,)),
        dma((3,)), dma((3,)),
        dma((3,)), dma((3,)),
        dma((xs - 1, 3)), dma((xs - 1, 3)),
        dma((xs, 3)), dma((xs, 3)),
        dma((ep_count,)), dma((ep_count,)),
        dma((2, zs)), dma((2, zs)),
        dma((6, zs)), dma((6, zs)),
        dma((ep_count,)), dma((ep_count,)),
        dma((3,)), dma((3,)),
    ]
    return pl.pallas_call(
        functools.partial(layer, dims=dims, cap=cap),
        out_shape=(
            jax.ShapeDtypeStruct((span, width), bf16),
            jax.ShapeDtypeStruct((rows, width), bf16),
        ),
        in_specs=[at_vmem] * 7 + [at_any] * 5,
        out_specs=(at_any, at_vmem),
        scratch_shapes=scratch,
        compiler_params=pltpu.CompilerParams(
            collective_id=0, has_side_effects=True, vmem_limit_bytes=60 * 1024 * 1024
        ),
    )(
        moe_input, moe_gain[None, :], routes.T, route_weights.T, conv_kernel, norm_gain[None, :],
        norm_shift[None, :], conv_input, conv_proj, gate_proj, up_proj, down_proj,
    )


def solution(mesh):
    placed = (
        P("ep", "tp"),
        P(None, "tp"),
        P("tp"),
        P("tp"),
        P("tp", None),
        P(("ep", "tp"), None),
        P(),
        P("ep", None),
        P("ep", None),
        P("ep", None, "tp"),
        P("ep", None, "tp"),
        P("ep", "tp", None),
    )
    return jax.shard_map(
        local,
        mesh=mesh,
        in_specs=placed,
        out_specs=(P(("ep", "tp"), None), P(("ep", "tp"), None)),
        check_vma=False,
    )
```

```python
import functools

import jax
import jax.numpy as jnp
from jax import lax
from jax.experimental import pallas as pl
from jax.experimental.pallas import tpu as pltpu
from jax.sharding import PartitionSpec as P

MESH = pl.DeviceIdType.MESH
DIMS = (8, 4, 2)
OFFSETS = {8: (0, 3, 5, 4, 2, 6, 1, 7), 4: (0, 2, 1, 3), 2: (0, 1)}
FAR = {8: (1, 4), 4: (1, 2), 2: (2, 2)}
ISSUE = {8: ((0,), (1, 2), (3,), (4, 5), (6, 7)), 4: ((0,), (1,), (2, 3)), 2: ((0,), (1,))}
f32, bf16, i32 = jnp.float32, jnp.bfloat16, jnp.int32


def layer(
    moe_in, moe_gain, routes, weights, taps_in, gain, shift, conv_hbm, proj_hbm, gate_hbm, up_hbm, down_hbm,
    conv_out, moe_out,
    padded, history, taps, affine_src, affine, mixed, xin, act, wfull,
    gate, up, down, own, group, ranks, held_w, scale, outgoing, arrived, pieces,
    moe_a, moe_b, moe_c, moe_d, moe_u, moe_v, back_out, returned, running, combined, final,
    load_sem, ready, hist_send, hist_recv, a2a_send, a2a_recv,
    cx_send, cx_recv, aff_send, aff_recv,
    wy_send, wy_recv, wx_send, wx_recv, wd_send, wd_recv, ep_send, ep_recv,
    gather_send, gather_recv, ret_send, ret_recv, back_send, back_recv, fin_send, fin_recv,
    *, dims, cap,
):
    zs, xs, cs = dims
    ep_count = zs * xs * cs
    per = xs * cs
    chunk = per * cap
    rows, width = moe_in.shape
    col = width // 4
    half = col // 2
    conv_rows = conv_hbm.shape[0]
    conv_width = conv_hbm.shape[1]
    reach = taps_in.shape[0] - 1
    lead = 32
    span = conv_rows // 4
    slice_cols = width // per

    me_ep, me = lax.axis_index("ep"), lax.axis_index("tp")
    core = lax.rem(me_ep, cs)
    mx = lax.rem(lax.div(me_ep, cs), xs)
    mz = lax.div(me_ep, cs * xs)
    nxt, prv = lax.rem(me + 1, 4), lax.rem(me + 3, 4)

    def remote(src, dst, send, recv, where):
        return pltpu.make_async_remote_copy(
            src_ref=src, dst_ref=dst, send_sem=send, recv_sem=recv, device_id=where,
            device_id_type=MESH,
        )

    def received(ref, sem):
        remote(ref, ref, sem, sem, {"tp": lax.rem(me + 1, 4)}).wait_recv()

    def gone(ref, sem):
        remote(ref, ref, sem, sem, {"tp": lax.rem(me + 1, 4)}).wait_send()

    def aligned(start, size):
        return pl.ds(pl.multiple_of(start, size), size)

    offsets = OFFSETS[zs]
    far_from, far_to = FAR[zs]

    def depth(c):
        return offsets[0] + sum(
            (offsets[k] - offsets[k - 1]) * lax.div(c + (zs - k), zs) for k in range(1, zs)
        )

    def place(z, x, c):
        return (z * xs + x) * cs + c

    def partner(c, j, way):
        dx, dc = j // cs, j % cs
        z = lax.rem(mz + way * depth(c) + zs, zs)
        x = lax.rem(mx + way * dx + xs, xs)
        return place(z, x, lax.rem(core + dc, cs))

    barrier = pltpu.get_barrier_semaphore()
    along_z = sorted(range(1, zs), key=lambda d: -min(d, zs - d))
    for d in along_z:
        pl.semaphore_signal(
            barrier, inc=1, device_id={"ep": place(lax.rem(mz + d, zs), mx, core)}, device_id_type=MESH
        )
    for k in (2, 1, 3):
        pl.semaphore_signal(barrier, inc=1, device_id={"tp": lax.rem(me + k, 4)}, device_id_type=MESH)
    for j in range(1, per):
        where = place(mz, lax.rem(mx + j // cs, xs), lax.rem(core + j % cs, cs))
        pl.semaphore_signal(barrier, inc=1, device_id={"ep": where}, device_id_type=MESH)

    loads = [pltpu.make_async_copy(conv_hbm, padded.at[lead:], load_sem.at[0])]
    for q in range(per):
        loads.append(
            pltpu.make_async_copy(
                proj_hbm.at[:, q * slice_cols : (q + 1) * slice_cols], wfull.at[q, me], load_sem.at[1]
            )
        )
    for k in range(4):
        at = lax.rem(me + k, 4) * col
        loads.append(pltpu.make_async_copy(gate_hbm.at[0, aligned(at, col), :], gate.at[k], load_sem.at[2]))
        loads.append(pltpu.make_async_copy(up_hbm.at[0, aligned(at, col), :], up.at[k], load_sem.at[3]))
        loads.append(pltpu.make_async_copy(down_hbm.at[0, :, aligned(at, col)], down.at[k], load_sem.at[4]))
    for load in loads:
        load.start()

    def loaded(ref, n):
        pltpu.make_async_copy(ref, ref, load_sem.at[n]).wait()

    value = moe_in[...].astype(f32)
    normed = (
        value * lax.rsqrt(jnp.mean(value * value, axis=1, keepdims=True) + 1e-06) * moe_gain[...]
    ).astype(bf16)
    for b in range(5):
        own[b] = normed[:, (b % 4) * col : (b % 4 + 1) * col]

    group_rows = routes.shape[1]
    s_at = lax.broadcasted_iota(i32, (ep_count, group_rows), 0)
    per_bits, core_bits = per.bit_length() - 1, cs.bit_length() - 1
    c_at = s_at >> per_bits
    dz = jnp.full_like(c_at, offsets[0])
    for k in range(1, zs):
        dz = jnp.where(c_at == k, offsets[k], dz)
    dx = (s_at & (per - 1)) >> core_bits
    dc = s_at & (cs - 1)
    expert = ((((mz + dz) & (zs - 1)) * xs + ((mx + dx) & (xs - 1))) * cs) + ((core + dc) & (cs - 1))
    first, second = routes[0:1, :] == expert, routes[1:2, :] == expert
    hit = first | second
    before = (
        lax.broadcasted_iota(i32, (group_rows, group_rows), 0)
        < lax.broadcasted_iota(i32, (group_rows, group_rows), 1)
    )
    rank = jnp.dot(
        jnp.where(hit, 1.0, 0.0).astype(bf16), jnp.where(before, 1.0, 0.0).astype(bf16),
        preferred_element_type=f32,
    )
    ranks[...] = jnp.where(hit, rank, -1.0)
    held_w[...] = jnp.where(first, weights[0:1, :], 0.0) + jnp.where(second, weights[1:2, :], 0.0)
    taps[0 : reach + 1, :] = taps_in[...].astype(f32)
    affine_src[0:1, :] = gain[...]
    affine_src[1:2, :] = shift[...]

    lane, strip = 128, min(64, span)

    def conv_strip(i, carry):
        at = aligned(i * strip, strip)
        r0 = pl.multiple_of(i * strip, strip)
        for n in range(0, conv_width, lane):
            x = padded[pl.ds(r0, strip + lead), n : n + lane].astype(f32)
            out = None
            for phase in range(8):
                acc = None
                extra = 8 if phase else 0
                for q in range(lead // 8 + 1):
                    tap = 8 * q + phase - (lead - reach)
                    if tap < 0 or tap > reach:
                        continue
                    term = x[8 * q : 8 * q + strip + extra] * taps[tap : tap + 1, n : n + lane]
                    acc = term if acc is None else acc + term
                if acc is None:
                    continue
                part = acc[phase : phase + strip]
                out = part if out is None else out + part
            mixed[at, n : n + lane] = out.astype(bf16)
        return carry

    strips = conv_rows // strip
    early = strips * 3 // 8
    loaded(padded.at[lead:], 0)
    lax.fori_loop(1, early, conv_strip, 0)

    pl.semaphore_wait(barrier, zs + per + 1)

    slice_id = mx * cs + core

    def w_first(k):
        piece = wfull.at[slice_id, me]
        return remote(piece, piece, wy_send, wy_recv.at[k - 1], {"tp": lax.rem(me + k, 4)})

    half_rows = conv_width // 2

    def w_relay(k):
        to, part = (nxt, slice(0, half_rows)) if k == 1 else (prv, slice(half_rows, conv_width))
        piece = wfull.at[slice_id, lax.rem(me + 4 - k, 4), part]
        return remote(piece, piece, wy_send, wy_recv.at[1], {"tp": to})

    a2a, conv_x, params = [], [], []
    for k in range(1, 4):
        to = lax.rem(me + k, 4)
        a2a.append(
            remote(
                own.at[pl.ds(to, 2)], group.at[:, aligned(me * rows, rows), :],
                a2a_send, a2a_recv, {"tp": to},
            )
        )
        for h in range(2):
            part = span // 2
            conv_x.append(
                remote(
                    mixed.at[aligned(to * span + h * part, part), :], xin.at[me, h * part : (h + 1) * part],
                    cx_send, cx_recv, {"tp": to},
                )
            )
        params.append(remote(affine_src, affine.at[me], aff_send, aff_recv, {"tp": to}))
    for r in a2a:
        r.start()
    loaded(wfull.at[:, 0], 1)
    for k in (1, 3):
        w_first(k).start()
    for d in along_z:
        pl.semaphore_signal(
            ready, inc=1, device_id={"ep": place(lax.rem(mz + d, zs), mx, core)}, device_id_type=MESH
        )
    group[:, aligned(me * rows, rows), :] = own[pl.ds(me, 2)]
    affine[me] = affine_src[...]
    lax.fori_loop(early, strips * 3 // 4, conv_strip, 0)
    pl.semaphore_wait(ready, zs - 1)
    hist = remote(
        padded.at[conv_rows : conv_rows + lead], history, hist_send, hist_recv,
        {"ep": lax.rem(me_ep + 1, ep_count)},
    )
    hist.start()
    lax.fori_loop(strips * 3 // 4, strips, conv_strip, 0)

    def normalise(i, carry):
        at = aligned(i * strip, strip)
        parts = [xin[b, at, :].astype(f32) for b in range(4)]
        one, two = sum(parts), sum(p * p for p in parts)
        center = jnp.sum(one, axis=1, keepdims=True) / width
        square = jnp.sum(two, axis=1, keepdims=True) / width
        inverse = lax.rsqrt(jnp.maximum(square - center * center, 0.0) + 1e-05)
        for b in range(4):
            scaled = (xin[b, at, :].astype(f32) - center) * inverse * affine[b, 0:1, :] + affine[b, 1:2, :]
            act[b, at, :] = (scaled / (1.0 + jnp.exp(-scaled))).astype(bf16)
        return carry

    def w_along(k, d):
        piece = wfull.at[slice_id, lax.rem(me + 4 - k, 4)]
        return remote(
            piece, piece, wx_send, wx_recv.at[k - 1],
            {"ep": place(mz, lax.rem(mx + d, xs), core)},
        )

    def w_across(k, d):
        piece = wfull.at[lax.rem(mx + xs - d, xs) * cs + core, lax.rem(me + 4 - k, 4)]
        return remote(
            piece, piece, wd_send, wd_recv,
            {"ep": place(mz, mx, lax.rem(core + 1, cs))},
        )

    def w_spread(k):
        if k == 2:
            received(wfull.at[0, 0], wy_recv.at[1])
        for d in range(1, xs):
            w_along(k, d).start()
        if cs > 1:
            w_across(k, 0).start()

    def w_share(k):
        received(wfull.at[0 : xs - 1, 0], wx_recv.at[k - 1])
        if cs > 1:
            for d in range(1, xs):
                w_across(k, d).start()

    def multiply(side):
        def one(d, carry):
            q = lax.rem(mx + d, xs) * cs + lax.rem(core + side, cs)
            total = sum(jnp.dot(act[b], wfull[q, b], preferred_element_type=f32) for b in range(4))
            conv_out[:, aligned(q * slice_cols, slice_cols)] = total.astype(bf16)
            return carry

        lax.fori_loop(0, xs, one, 0)

    received(group.at[:, 0 : 3 * rows, :], a2a_recv)
    for r in params:
        r.start()

    slot = lax.broadcasted_iota(i32, (cap, group_rows), 0).astype(f32)

    def ep_copy(c, j):
        s = c * per + j
        blocks = slice(0, 1 if far_from <= c < far_to else 2)
        return remote(
            outgoing.at[blocks, aligned(s * cap, cap), :],
            arrived.at[blocks, aligned(s * cap, cap), :],
            ep_send, ep_recv.at[c], {"ep": partner(c, j, 1)},
        )

    def dispatch(group_of):
        for c in group_of:
            ranked = ranks[c * per : (c + 1) * per, :]
            pick = jnp.concatenate(
                [jnp.where(ranked[j : j + 1, :] == slot, 1.0, 0.0) for j in range(per)], axis=0
            ).astype(bf16)
            for b in range(1 if far_from <= c < far_to else 2):
                outgoing[b, c * chunk : (c + 1) * chunk, :] = jnp.dot(
                    pick, group[b], preferred_element_type=f32
                ).astype(bf16)
        for j in range(per):
            for c in group_of:
                if (c, j) != (0, 0):
                    ep_copy(c, j).start()

    for group_of in ISSUE[zs]:
        dispatch(group_of)
    mine = slice(0, cap)
    arrived[0:2, mine, :] = outgoing[:, mine, :]

    hist.wait_recv()
    padded[0:lead, :] = jnp.where(me_ep == 0, jnp.zeros((lead, conv_width), bf16), history[...])
    lax.fori_loop(0, 1, conv_strip, 0)
    xin[me] = mixed[aligned(me * span, span), :]

    def weigh(c, carry):
        ranked = ranks[aligned(c * per, per), :]
        held = held_w[aligned(c * per, per), :]
        block = jnp.concatenate(
            [jnp.where(ranked[j : j + 1, :] == slot, held[j : j + 1, :], 0.0) for j in range(per)], axis=0
        )
        scale[c] = block.T.astype(bf16)
        return carry

    lax.fori_loop(0, zs, weigh, 0)

    def is_far(c):
        return (c >= far_from) & (c < far_to)

    def gather_copy(n, c):
        at = aligned(c * chunk, chunk)
        low, high = slice(0, half), slice(half, col)
        src, dst, where = [
            (arrived.at[1, at, :], arrived.at[2, at, :], prv),
            (arrived.at[0, at, :], arrived.at[3, at, :], nxt),
            (arrived.at[0, at, :], arrived.at[1, at, :], prv),
            (arrived.at[1, at, low], arrived.at[2, at, low], prv),
            (arrived.at[3, at, high], arrived.at[2, at, high], nxt),
        ][n]
        sem = (0, 1, 0, 2, 2)[n]
        return remote(src, dst, gather_send.at[sem], gather_recv.at[sem, c], {"tp": where})

    def land(c):
        at = aligned(c * chunk, chunk)

        @pl.when(c == 0)
        def _():
            received(arrived.at[0:2, 0 : chunk - cap, :], ep_recv.at[c])

        @pl.when((c > 0) & jnp.logical_not(is_far(c)))
        def _():
            received(arrived.at[0:2, at, :], ep_recv.at[c])

        @pl.when(is_far(c))
        def _():
            received(arrived.at[0, at, :], ep_recv.at[c])
            gather_copy(2, c).start()

        @pl.when(jnp.logical_not(is_far(c)))
        def _():
            gather_copy(0, c).start()

        gather_copy(1, c).start()

    def relay(c):
        at = aligned(c * chunk, chunk)
        received(arrived.at[1, at, :], gather_recv.at[0, c])
        gather_copy(3, c).start()
        received(arrived.at[3, at, :], gather_recv.at[1, c])
        gather_copy(4, c).start()

    def return_copies(c):
        at = aligned(c * chunk, chunk)
        low, high = slice(0, half), slice(half, col)

        def one(n, src, dst, where):
            return remote(src, dst, ret_send.at[n], ret_recv.at[n, c], {"tp": where})

        return [
            one(0, pieces.at[2, at, low], moe_a.at[at, :], nxt),
            one(1, pieces.at[2, at, high], moe_b.at[at, :], prv),
            one(2, pieces.at[1, at, high], moe_c.at[at, high], nxt),
            one(3, pieces.at[3, at, low], moe_d.at[at, low], prv),
            one(2, moe_u.at[at, :], moe_c.at[at, low], nxt),
            one(3, moe_v.at[at, :], moe_d.at[at, high], prv),
        ]

    def experts(c):
        at = aligned(c * chunk, chunk)

        @pl.when(is_far(c))
        def _():
            received(arrived.at[2, at, :], gather_recv.at[2, c])

        @pl.when(jnp.logical_not(is_far(c)))
        def _():
            received(arrived.at[2, at, :], gather_recv.at[0, c])
            received(arrived.at[3, at, :], gather_recv.at[1, c])

        lines = [arrived[k, at, :] for k in range(4)]
        hidden = []
        step = min(256, col)
        for n in range(0, col, step):
            left = sum(jnp.dot(lines[k], gate[k, :, n : n + step], preferred_element_type=f32) for k in range(4))
            right = sum(jnp.dot(lines[k], up[k, :, n : n + step], preferred_element_type=f32) for k in range(4))
            hidden.append((left / (1.0 + jnp.exp(-left)) * right).astype(bf16))
        hid = jnp.concatenate(hidden, axis=1)
        for k in (2, 1, 3, 0):
            pieces[k, at, :] = jnp.dot(hid, down[k], preferred_element_type=f32).astype(bf16)
        for r in return_copies(c)[:4]:
            r.start()

    def middle(c):
        copies = return_copies(c)
        at = aligned(c * chunk, chunk)
        copies[0].wait_recv()
        moe_u[at, :] = (pieces[1, at, :half].astype(f32) + moe_a[at, :].astype(f32)).astype(bf16)
        copies[4].start()
        copies[1].wait_recv()
        moe_v[at, :] = (pieces[3, at, half:].astype(f32) + moe_b[at, :].astype(f32)).astype(bf16)
        copies[5].start()

    def back_copy(c, j):
        s = c * per + j
        at = aligned(s * cap, cap)
        return remote(
            back_out.at[at, :], returned.at[at, :], back_send, back_recv.at[c],
            {"ep": partner(c, j, -1)},
        )

    def finish(c):
        at = aligned(c * chunk, chunk)
        received(moe_c.at[at, :], ret_recv.at[2, c])
        received(moe_d.at[at, :], ret_recv.at[3, c])
        back_out[at, :] = (
            pieces[0, at, :].astype(f32) + moe_c[at, :].astype(f32) + moe_d[at, :].astype(f32)
        ).astype(bf16)
        for j in range(per):
            if j == 0:
                @pl.when(c > 0)
                def _():
                    back_copy(c, 0).start()
            else:
                back_copy(c, j).start()

    for k in (1, 3):
        received(wfull.at[0, 0], wy_recv.at[k - 1])
        w_relay(k).start()
    land(0)

    def step(i, carry):
        @pl.when((i >= 3) & (i + 2 < zs))
        def _():
            land(i + 2)

        for n in (1, 2):
            if far_from <= n < far_to:
                @pl.when(i == 1)
                def _():
                    relay(n)

        @pl.when(i == 0)
        def _():
            loaded(gate, 2)
            loaded(up, 3)
            loaded(down, 4)

        experts(i)

        for n in range(max(far_from, 3), far_to):
            @pl.when(i == n - 1)
            def _():
                relay(n)

        @pl.when(i >= 1)
        def _():
            middle(i - 1)

        @pl.when(i >= 2)
        def _():
            finish(i - 2)

        for n, k in enumerate((1, 3, 2)):
            @pl.when(i == spread_at[n])
            def _():
                w_spread(k)

            @pl.when(i == share_at[n])
            def _():
                w_share(k)

        for n, at_end in ((1, 0), (2, 0), (3, 1), (4, 2)):
            if n < zs:
                @pl.when(i == at_end)
                def _():
                    land(n)

        return carry

    spread_at = [min(n, zs - 1) for n in (0, 1, 2)]
    share_at = [min(n, zs - 1) for n in (5, 6, 7)]
    lax.fori_loop(0, zs, step, 0)
    middle(zs - 1)
    finish(zs - 2)
    for r in conv_x:
        r.start()
    finish(zs - 1)

    returned[mine, :] = back_out[mine, :]
    def combine(c):
        here = slice(c * chunk + (0 if c else cap), (c + 1) * chunk)
        received(returned.at[here, :], back_recv.at[c])
        return jnp.dot(scale[c], returned[c * chunk : (c + 1) * chunk, :], preferred_element_type=f32)

    total = combine(0)
    for c in range(1, zs - 1):
        total = total + combine(c)
    running[...] = total
    total = running[...] + combine(zs - 1)
    combined[...] = total.astype(bf16)
    last = []
    for k in range(1, 4):
        to = lax.rem(me + k, 4)
        last.append(
            remote(
                combined.at[aligned(to * rows, rows), :], final.at[me],
                fin_send, fin_recv, {"tp": to},
            )
        )
    for r in last:
        r.start()
    final[me] = combined[aligned(me * rows, rows), :]
    received(affine.at[0:3], aff_recv)
    received(xin.at[0:3], cx_recv)
    lax.fori_loop(0, span // strip, normalise, 0)
    multiply(0)
    if cs > 1:
        received(wfull.at[0:xs, 0:3], wd_recv)
        multiply(1)
    received(final.at[0:3], fin_recv)
    for b in range(4):
        moe_out[:, b * col : (b + 1) * col] = final[b]

    gone(own.at[0:6], a2a_send)
    gone(xin.at[0:3], cx_send)
    gone(affine.at[0:3], aff_send)
    hist.wait_send()
    gone(wfull.at[0:3, 0], wy_send)
    gone(wfull.at[0 : xs - 1, 0:3], wx_send)
    if cs > 1:
        gone(wfull.at[0:xs, 0:3], wd_send)
    sent = (2 * (zs - far_to + far_from) + far_to - far_from) * chunk // 2 - cap
    gone(outgoing.at[:, 0:sent, :], ep_send)
    gone(arrived.at[0], gather_send.at[0])
    gone(arrived.at[0], gather_send.at[1])
    if far_to > far_from:
        gone(arrived.at[0, 0 : (far_to - far_from) * chunk], gather_send.at[2])
    gone(moe_a, ret_send.at[0])
    gone(moe_b, ret_send.at[1])
    gone(moe_c, ret_send.at[2])
    gone(moe_d, ret_send.at[3])
    gone(back_out.at[cap:, :], back_send)
    gone(final.at[0:3], fin_send)


def local(
    conv_input, conv_kernel, norm_gain, norm_shift, conv_proj, moe_input, moe_gain,
    routes, route_weights, gate_proj, up_proj, down_proj, *, dims=DIMS,
):
    zs, xs, cs = dims
    ep_count = zs * xs * cs
    conv_rows, conv_width = conv_input.shape
    rows, width = moe_input.shape
    group_rows = routes.shape[0]
    cap = 16
    slots = ep_count * cap
    col, half = width // 4, width // 8
    span = conv_rows // 4
    hid = gate_proj.shape[2]
    chunk = xs * cs * cap
    per = xs * cs
    vmem, dma = pltpu.VMEM, pltpu.SemaphoreType.DMA
    at_vmem, at_hbm = pl.BlockSpec(memory_space=pltpu.VMEM), pl.BlockSpec(memory_space=pltpu.HBM)
    scratch = [
        vmem((32 + conv_rows, conv_width), bf16),
        vmem((32, conv_width), bf16),
        vmem((32, conv_width), f32),
        vmem((2, conv_width), f32),
        vmem((4, 2, conv_width), f32),
        vmem((conv_rows, conv_width), bf16),
        vmem((4, span, conv_width), bf16),
        vmem((4, span, conv_width), bf16),
        vmem((per, 4, conv_width, width // per), bf16),
        vmem((4, col, hid), bf16), vmem((4, col, hid), bf16), vmem((4, hid, col), bf16),
        vmem((6, rows, col), bf16),
        vmem((2, group_rows, col), bf16),
        vmem((ep_count, group_rows), f32), vmem((ep_count, group_rows), f32),
        vmem((zs, group_rows, chunk), bf16),
        vmem((2, slots, col), bf16),
        vmem((4, slots, col), bf16),
        vmem((4, slots, col), bf16),
        vmem((slots, half), bf16), vmem((slots, half), bf16),
        vmem((slots, col), bf16), vmem((slots, col), bf16),
        vmem((slots, half), bf16), vmem((slots, half), bf16),
        vmem((slots, col), bf16), vmem((slots, col), bf16),
        vmem((group_rows, col), f32),
        vmem((group_rows, col), bf16),
        vmem((4, rows, col), bf16),
        dma((5,)), pltpu.SemaphoreType.REGULAR,
        dma, dma,
        dma, dma,
        dma, dma,
        dma, dma,
        dma, dma((3,)),
        dma, dma((3,)),
        dma, dma,
        dma, dma((zs,)),
        dma((3,)), dma((3, zs)),
        dma((4,)), dma((4, zs)),
        dma, dma((zs,)),
        dma, dma,
    ]
    return pl.pallas_call(
        functools.partial(layer, dims=dims, cap=cap),
        out_shape=(
            jax.ShapeDtypeStruct((span, width), bf16),
            jax.ShapeDtypeStruct((rows, width), bf16),
        ),
        in_specs=[at_vmem] * 7 + [at_hbm] * 5,
        out_specs=(at_vmem, at_vmem),
        scratch_shapes=scratch,
        compiler_params=pltpu.CompilerParams(
            collective_id=0, has_side_effects=True, vmem_limit_bytes=60 * 1024 * 1024
        ),
    )(
        moe_input, moe_gain[None, :], routes.T, route_weights.T, conv_kernel, norm_gain[None, :],
        norm_shift[None, :], conv_input, conv_proj, gate_proj, up_proj, down_proj,
    )


def solution(mesh):
    placed = (
        P("ep", "tp"),
        P(None, "tp"),
        P("tp"),
        P("tp"),
        P("tp", None),
        P(("ep", "tp"), None),
        P(),
        P("ep", None),
        P("ep", None),
        P("ep", None, "tp"),
        P("ep", None, "tp"),
        P("ep", "tp", None),
    )
    return jax.shard_map(
        local,
        mesh=mesh,
        in_specs=placed,
        out_specs=(P(("ep", "tp"), None), P(("ep", "tp"), None)),
        check_vma=False,
    )
```

```python
import functools

import jax
import jax.numpy as jnp
from jax import lax
from jax.experimental import pallas as pl
from jax.experimental.pallas import tpu as pltpu
from jax.sharding import PartitionSpec as P

MESH = pl.DeviceIdType.MESH
DIMS = (8, 4, 2)
OFFSETS = {8: (0, 3, 5, 4, 2, 6, 1, 7), 4: (0, 2, 1, 3), 2: (0, 1)}
FAR = {8: (1, 4), 4: (1, 2), 2: (2, 2)}
ISSUE = {8: ((0,), (1, 2), (3,), (4, 5), (6, 7)), 4: ((0,), (1,), (2, 3)), 2: ((0,), (1,))}
f32, bf16, i32 = jnp.float32, jnp.bfloat16, jnp.int32


def layer(
    moe_in, moe_gain, routes, weights, taps_in, gain, shift, conv_hbm, proj_hbm, gate_hbm, up_hbm, down_hbm,
    conv_out, moe_out,
    padded, history, taps, mixed, sums, stats, stats_in, columns, active, xin, conv_sum, wfull,
    gate, up, down, own, group, ranks, held_w, scale, outgoing, arrived, pieces,
    moe_a, moe_b, moe_c, moe_d, moe_u, moe_v, back_out, returned, running, combined, final,
    load_sem, ready, hist_send, hist_recv, a2a_send, a2a_recv,
    cx_send, cx_recv, stat_send, stat_recv,
    wy_send, wy_recv, wz_send, wz_recv, wx_send, wx_recv, wd_send, wd_recv, ep_send, ep_recv,
    gather_send, gather_recv, ret_send, ret_recv, back_send, back_recv, fin_send, fin_recv,
    *, dims, cap,
):
    zs, xs, cs = dims
    ep_count = zs * xs * cs
    per = xs * cs
    chunk = per * cap
    rows, width = moe_in.shape
    col = width // 4
    half = col // 2
    conv_rows = conv_hbm.shape[0]
    conv_width = conv_hbm.shape[1]
    reach = taps_in.shape[0] - 1
    lead = 32
    span = conv_rows // 4
    slice_cols = width // per

    me_ep, me = lax.axis_index("ep"), lax.axis_index("tp")
    core = lax.rem(me_ep, cs)
    mx = lax.rem(lax.div(me_ep, cs), xs)
    mz = lax.div(me_ep, cs * xs)
    nxt, opp, prv = lax.rem(me + 1, 4), lax.rem(me + 2, 4), lax.rem(me + 3, 4)

    def remote(src, dst, send, recv, where):
        return pltpu.make_async_remote_copy(
            src_ref=src, dst_ref=dst, send_sem=send, recv_sem=recv, device_id=where,
            device_id_type=MESH,
        )

    def received(ref, sem):
        remote(ref, ref, sem, sem, {"tp": lax.rem(me + 1, 4)}).wait_recv()

    def gone(ref, sem):
        remote(ref, ref, sem, sem, {"tp": lax.rem(me + 1, 4)}).wait_send()

    def aligned(start, size):
        return pl.ds(pl.multiple_of(start, size), size)

    offsets = OFFSETS[zs]
    far_from, far_to = FAR[zs]

    def depth(c):
        return offsets[0] + sum(
            (offsets[k] - offsets[k - 1]) * lax.div(c + (zs - k), zs) for k in range(1, zs)
        )

    def place(z, x, c):
        return (z * xs + x) * cs + c

    def partner(c, j, way):
        dx, dc = j // cs, j % cs
        z = lax.rem(mz + way * depth(c) + zs, zs)
        x = lax.rem(mx + way * dx + xs, xs)
        return place(z, x, lax.rem(core + dc, cs))

    barrier = pltpu.get_barrier_semaphore()
    along_z = sorted(range(1, zs), key=lambda d: -min(d, zs - d))
    for d in along_z:
        pl.semaphore_signal(
            barrier, inc=1, device_id={"ep": place(lax.rem(mz + d, zs), mx, core)}, device_id_type=MESH
        )
    for k in (2, 1, 3):
        pl.semaphore_signal(barrier, inc=1, device_id={"tp": lax.rem(me + k, 4)}, device_id_type=MESH)
    for j in range(1, per):
        where = place(mz, lax.rem(mx + j // cs, xs), lax.rem(core + j % cs, cs))
        pl.semaphore_signal(barrier, inc=1, device_id={"ep": where}, device_id_type=MESH)

    loads = [pltpu.make_async_copy(conv_hbm, padded.at[lead:], load_sem.at[0])]
    for q in range(per):
        loads.append(
            pltpu.make_async_copy(
                proj_hbm.at[:, q * slice_cols : (q + 1) * slice_cols], wfull.at[q, me], load_sem.at[1]
            )
        )
    for k in range(4):
        at = lax.rem(me + k, 4) * col
        loads.append(pltpu.make_async_copy(gate_hbm.at[0, aligned(at, col), :], gate.at[k], load_sem.at[2]))
        loads.append(pltpu.make_async_copy(up_hbm.at[0, aligned(at, col), :], up.at[k], load_sem.at[3]))
        loads.append(pltpu.make_async_copy(down_hbm.at[0, :, aligned(at, col)], down.at[k], load_sem.at[4]))
    for load in loads:
        load.start()

    def loaded(ref, n):
        pltpu.make_async_copy(ref, ref, load_sem.at[n]).wait()

    value = moe_in[...].astype(f32)
    normed = (
        value * lax.rsqrt(jnp.mean(value * value, axis=1, keepdims=True) + 1e-06) * moe_gain[...]
    ).astype(bf16)
    for b in range(5):
        own[b] = normed[:, (b % 4) * col : (b % 4 + 1) * col]

    group_rows = routes.shape[1]
    s_at = lax.broadcasted_iota(i32, (ep_count, group_rows), 0)
    per_bits, core_bits = per.bit_length() - 1, cs.bit_length() - 1
    c_at = s_at >> per_bits
    dz = jnp.full_like(c_at, offsets[0])
    for k in range(1, zs):
        dz = jnp.where(c_at == k, offsets[k], dz)
    dx = (s_at & (per - 1)) >> core_bits
    dc = s_at & (cs - 1)
    expert = ((((mz + dz) & (zs - 1)) * xs + ((mx + dx) & (xs - 1))) * cs) + ((core + dc) & (cs - 1))
    first, second = routes[0:1, :] == expert, routes[1:2, :] == expert
    hit = first | second
    before = (
        lax.broadcasted_iota(i32, (group_rows, group_rows), 0)
        < lax.broadcasted_iota(i32, (group_rows, group_rows), 1)
    )
    rank = jnp.dot(
        jnp.where(hit, 1.0, 0.0).astype(bf16), jnp.where(before, 1.0, 0.0).astype(bf16),
        preferred_element_type=f32,
    )
    ranks[...] = jnp.where(hit, rank, -1.0)
    held_w[...] = jnp.where(first, weights[0:1, :], 0.0) + jnp.where(second, weights[1:2, :], 0.0)
    taps[0 : reach + 1, :] = taps_in[...].astype(f32)

    tile = span // 2
    tiles = conv_rows // tile
    lane, strip = 128, min(64, tile)

    def conv_tile(i, carry):
        for h in range(tile // strip):
            r0 = pl.multiple_of(i * tile + h * strip, strip)
            one = jnp.zeros((strip, lane), f32)
            two = jnp.zeros((strip, lane), f32)
            for n in range(0, conv_width, lane):
                x = padded[pl.ds(r0, strip + lead), n : n + lane].astype(f32)
                out = None
                for phase in range(8):
                    acc = None
                    extra = 8 if phase else 0
                    for q in range(lead // 8 + 1):
                        tap = 8 * q + phase - (lead - reach)
                        if tap < 0 or tap > reach:
                            continue
                        term = x[8 * q : 8 * q + strip + extra] * taps[tap : tap + 1, n : n + lane]
                        acc = term if acc is None else acc + term
                    if acc is None:
                        continue
                    part = acc[phase : phase + strip]
                    out = part if out is None else out + part
                mixed[pl.ds(r0, strip), n : n + lane] = out
                one = one + out
                two = two + out * out
            sums[0, h * strip : (h + 1) * strip, :] = one
            sums[1, h * strip : (h + 1) * strip, :] = two
        for m in range(2):
            stats[m, pl.ds(i, 1), :] = jnp.sum(sums[m].T, axis=0, keepdims=True)
        return carry

    early = tiles * 3 // 8
    loaded(padded.at[lead:], 0)
    lax.fori_loop(1, early, conv_tile, 0)

    pl.semaphore_wait(barrier, zs + per + 1)

    slice_id = mx * cs + core

    own_rows = conv_width // 2
    parity = lax.rem(mz, 2)
    half_rows = own_rows // 2

    def w_first(k):
        piece = wfull.at[slice_id, me, aligned(parity * own_rows, own_rows)]
        return remote(piece, piece, wy_send, wy_recv.at[k - 1], {"tp": lax.rem(me + k, 4)})

    def w_relay(k):
        to, part = (nxt, 0) if k == 1 else (prv, half_rows)
        rows_at = aligned(parity * own_rows + part, half_rows)
        piece = wfull.at[slice_id, lax.rem(me + 4 - k, 4), rows_at]
        return remote(piece, piece, wy_send, wy_recv.at[1], {"tp": to})

    def w_pair(k):
        piece = wfull.at[slice_id, lax.rem(me + 4 - k, 4), aligned(parity * own_rows, own_rows)]
        where = place(mz + 1 - 2 * parity, mx, core)
        return remote(piece, piece, wz_send, wz_recv.at[k - 1], {"ep": where})

    a2a, conv_x, moments = [], [], []
    for k in range(1, 4):
        to = lax.rem(me + k, 4)
        a2a.append(
            remote(
                own.at[pl.ds(to, 2)], group.at[:, aligned(me * rows, rows), :],
                a2a_send, a2a_recv, {"tp": to},
            )
        )
        conv_x.append(
            remote(
                active.at[aligned(to * span, span), :], xin.at[me], cx_send, cx_recv.at[k - 1], {"tp": to},
            )
        )
        moments.append(remote(stats, stats_in.at[k - 1], stat_send, stat_recv, {"tp": to}))
    for r in a2a:
        r.start()
    for d in along_z:
        pl.semaphore_signal(
            ready, inc=1, device_id={"ep": place(lax.rem(mz + d, zs), mx, core)}, device_id_type=MESH
        )
    group[:, aligned(me * rows, rows), :] = own[pl.ds(me, 2)]
    lax.fori_loop(early, tiles * 3 // 4, conv_tile, 0)
    pl.semaphore_wait(ready, zs - 1)
    hist = remote(
        padded.at[conv_rows : conv_rows + lead], history, hist_send, hist_recv,
        {"ep": lax.rem(me_ep + 1, ep_count)},
    )
    hist.start()
    lax.fori_loop(tiles * 3 // 4, tiles, conv_tile, 0)

    def center_and_scale():
        received(stats_in, stat_recv)
        total = (stats[...] + stats_in[0] + stats_in[1] + stats_in[2]) / width
        center = total[0]
        spread = jnp.maximum(total[1] - center * center, 0.0)
        inverse = lax.rsqrt(spread + 1e-05)
        for i in range(tiles):
            both = jnp.concatenate([center[i : i + 1], inverse[i : i + 1]] + [center[i : i + 1]] * 6, axis=0)
            columns[i * tile : (i + 1) * tile, :] = both.T

    def activate(i, carry):
        view = aligned(i * strip, strip)
        stat = columns[view, :]
        scaled = (mixed[view, :] - stat[:, 0:1]) * stat[:, 1:2] * gain[...] + shift[...]
        active[view, :] = (scaled / (1.0 + jnp.exp(-scaled))).astype(bf16)
        return carry

    ends = (1, xs - 1) if xs > 2 else (1,)

    def w_along(k, d):
        piece = wfull.at[slice_id, lax.rem(me + 4 - k, 4)]
        return remote(
            piece, piece, wx_send, wx_recv.at[0 if d == 1 else 1, k - 1],
            {"ep": place(mz, lax.rem(mx + d, xs), core)},
        )

    def w_onward(k, d):
        at = 0 if d == 1 else own_rows
        piece = wfull.at[lax.rem(mx + xs - d, xs) * cs + core, lax.rem(me + 4 - k, 4), at : at + own_rows]
        return remote(
            piece, piece, wx_send, wx_recv.at[2, k - 1],
            {"ep": place(mz, lax.rem(mx + d, xs), core)},
        )

    def w_across(k, d):
        piece = wfull.at[lax.rem(mx + xs - d, xs) * cs + core, lax.rem(me + 4 - k, 4)]
        return remote(
            piece, piece, wd_send, wd_recv,
            {"ep": place(mz, mx, lax.rem(core + 1, cs))},
        )

    def w_spread(k):
        received(wfull.at[0, 0, 0:own_rows], wz_recv.at[k - 1])
        for d in ends:
            w_along(k, d).start()
        if cs > 1:
            w_across(k, 0).start()

    def w_hop(k):
        for n, d in enumerate(ends):
            received(wfull.at[0, 0], wx_recv.at[n, k - 1])
            if xs > 2:
                w_onward(k, d).start()
            if cs > 1:
                w_across(k, d).start()

    def w_share(k):
        if xs > 2:
            received(wfull.at[0, 0], wx_recv.at[2, k - 1])
            if cs > 1:
                w_across(k, 2).start()

    def multiply(q, carry):
        total = sum(
            jnp.dot(xin[b], wfull[q, b], preferred_element_type=f32) for b in (me, prv, nxt)
        )
        conv_sum[q] = total
        return carry

    def multiply_last(q, carry):
        total = conv_sum[q] + jnp.dot(xin[opp], wfull[q, opp], preferred_element_type=f32)
        conv_out[:, aligned(q * slice_cols, slice_cols)] = total.astype(bf16)
        return carry

    received(group.at[:, 0 : 3 * rows, :], a2a_recv)
    loaded(wfull.at[:, 0], 1)
    for k in (1, 3):
        w_first(k).start()

    slot = lax.broadcasted_iota(i32, (cap, group_rows), 0).astype(f32)

    def ep_copy(c, j):
        s = c * per + j
        blocks = slice(0, 1 if far_from <= c < far_to else 2)
        return remote(
            outgoing.at[blocks, aligned(s * cap, cap), :],
            arrived.at[blocks, aligned(s * cap, cap), :],
            ep_send, ep_recv.at[c], {"ep": partner(c, j, 1)},
        )

    def dispatch(group_of):
        for c in group_of:
            ranked = ranks[c * per : (c + 1) * per, :]
            pick = jnp.concatenate(
                [jnp.where(ranked[j : j + 1, :] == slot, 1.0, 0.0) for j in range(per)], axis=0
            ).astype(bf16)
            for b in range(1 if far_from <= c < far_to else 2):
                outgoing[b, c * chunk : (c + 1) * chunk, :] = jnp.dot(
                    pick, group[b], preferred_element_type=f32
                ).astype(bf16)
        for j in range(per):
            for c in group_of:
                if (c, j) != (0, 0):
                    ep_copy(c, j).start()

    for group_of in ISSUE[zs]:
        dispatch(group_of)
    mine = slice(0, cap)
    arrived[0:2, mine, :] = outgoing[:, mine, :]

    hist.wait_recv()
    padded[0:lead, :] = jnp.where(me_ep == 0, jnp.zeros((lead, conv_width), bf16), history[...])
    lax.fori_loop(0, 1, conv_tile, 0)
    for r in moments:
        r.start()

    def weigh(c, carry):
        ranked = ranks[aligned(c * per, per), :]
        held = held_w[aligned(c * per, per), :]
        block = jnp.concatenate(
            [jnp.where(ranked[j : j + 1, :] == slot, held[j : j + 1, :], 0.0) for j in range(per)], axis=0
        )
        scale[c] = block.T.astype(bf16)
        return carry

    lax.fori_loop(0, zs, weigh, 0)

    def is_far(c):
        return (c >= far_from) & (c < far_to)

    def gather_copy(n, c):
        at = aligned(c * chunk, chunk)
        low, high = slice(0, half), slice(half, col)
        src, dst, where = [
            (arrived.at[1, at, :], arrived.at[2, at, :], prv),
            (arrived.at[0, at, :], arrived.at[3, at, :], nxt),
            (arrived.at[0, at, :], arrived.at[1, at, :], prv),
            (arrived.at[1, at, low], arrived.at[2, at, low], prv),
            (arrived.at[3, at, high], arrived.at[2, at, high], nxt),
        ][n]
        sem = (0, 1, 0, 2, 2)[n]
        return remote(src, dst, gather_send.at[sem], gather_recv.at[sem, c], {"tp": where})

    def land(c):
        at = aligned(c * chunk, chunk)

        @pl.when(c == 0)
        def _():
            received(arrived.at[0:2, 0 : chunk - cap, :], ep_recv.at[c])

        @pl.when((c > 0) & jnp.logical_not(is_far(c)))
        def _():
            received(arrived.at[0:2, at, :], ep_recv.at[c])

        @pl.when(is_far(c))
        def _():
            received(arrived.at[0, at, :], ep_recv.at[c])
            gather_copy(2, c).start()

        @pl.when(jnp.logical_not(is_far(c)))
        def _():
            gather_copy(0, c).start()

        gather_copy(1, c).start()

    def relay(c):
        at = aligned(c * chunk, chunk)
        received(arrived.at[1, at, :], gather_recv.at[0, c])
        gather_copy(3, c).start()
        received(arrived.at[3, at, :], gather_recv.at[1, c])
        gather_copy(4, c).start()

    def return_copies(c):
        at = aligned(c * chunk, chunk)
        low, high = slice(0, half), slice(half, col)

        def one(n, src, dst, where):
            return remote(src, dst, ret_send.at[n], ret_recv.at[n, c], {"tp": where})

        return [
            one(0, pieces.at[2, at, low], moe_a.at[at, :], nxt),
            one(1, pieces.at[2, at, high], moe_b.at[at, :], prv),
            one(2, pieces.at[1, at, high], moe_c.at[at, high], nxt),
            one(3, pieces.at[3, at, low], moe_d.at[at, low], prv),
            one(2, moe_u.at[at, :], moe_c.at[at, low], nxt),
            one(3, moe_v.at[at, :], moe_d.at[at, high], prv),
        ]

    def experts(c):
        at = aligned(c * chunk, chunk)

        @pl.when(is_far(c))
        def _():
            received(arrived.at[2, at, :], gather_recv.at[2, c])

        @pl.when(jnp.logical_not(is_far(c)))
        def _():
            received(arrived.at[2, at, :], gather_recv.at[0, c])
            received(arrived.at[3, at, :], gather_recv.at[1, c])

        lines = [arrived[k, at, :] for k in range(4)]
        hidden = []
        step = min(256, col)
        for n in range(0, col, step):
            left = sum(jnp.dot(lines[k], gate[k, :, n : n + step], preferred_element_type=f32) for k in range(4))
            right = sum(jnp.dot(lines[k], up[k, :, n : n + step], preferred_element_type=f32) for k in range(4))
            hidden.append((left / (1.0 + jnp.exp(-left)) * right).astype(bf16))
        hid = jnp.concatenate(hidden, axis=1)
        for k in (2, 1, 3, 0):
            pieces[k, at, :] = jnp.dot(hid, down[k], preferred_element_type=f32).astype(bf16)
        for r in return_copies(c)[:4]:
            r.start()

    def middle(c):
        copies = return_copies(c)
        at = aligned(c * chunk, chunk)
        copies[0].wait_recv()
        moe_u[at, :] = (pieces[1, at, :half].astype(f32) + moe_a[at, :].astype(f32)).astype(bf16)
        copies[4].start()
        copies[1].wait_recv()
        moe_v[at, :] = (pieces[3, at, half:].astype(f32) + moe_b[at, :].astype(f32)).astype(bf16)
        copies[5].start()

    def back_copy(c, j):
        s = c * per + j
        at = aligned(s * cap, cap)
        return remote(
            back_out.at[at, :], returned.at[at, :], back_send, back_recv.at[c],
            {"ep": partner(c, j, -1)},
        )

    def finish(c):
        at = aligned(c * chunk, chunk)
        received(moe_c.at[at, :], ret_recv.at[2, c])
        received(moe_d.at[at, :], ret_recv.at[3, c])
        back_out[at, :] = (
            pieces[0, at, :].astype(f32) + moe_c[at, :].astype(f32) + moe_d[at, :].astype(f32)
        ).astype(bf16)
        for j in range(per):
            if j == 0:
                @pl.when(c > 0)
                def _():
                    back_copy(c, 0).start()
            else:
                back_copy(c, j).start()

    land(0)
    for k in (1, 3):
        received(wfull.at[0, 0, 0:own_rows], wy_recv.at[k - 1])
        w_relay(k).start()
        w_pair(k).start()

    def step(i, carry):
        @pl.when((i >= 3) & (i + 2 < zs))
        def _():
            land(i + 2)

        for n in (1, 2):
            if far_from <= n < far_to:
                @pl.when(i == 1)
                def _():
                    relay(n)

        @pl.when(i == 0)
        def _():
            loaded(gate, 2)
            loaded(up, 3)
            loaded(down, 4)

        experts(i)

        for n in range(max(far_from, 3), far_to):
            @pl.when(i == n - 1)
            def _():
                relay(n)

        @pl.when(i >= 1)
        def _():
            middle(i - 1)

        @pl.when(i >= 2)
        def _():
            finish(i - 2)

        @pl.when(i == 0)
        def _():
            center_and_scale()
            lax.fori_loop(0, conv_rows // strip, activate, 0)
            xin[me] = active[aligned(me * span, span), :]
            received(wfull.at[0, 0, 0:own_rows], wy_recv.at[1])
            w_pair(2).start()

        for n, k in enumerate((1, 3, 2)):
            @pl.when(i == spread_at[n])
            def _():
                w_spread(k)

            @pl.when(i == hop_at[n])
            def _():
                w_hop(k)

        for n, at_end in ((1, 0), (2, 0), (3, 1), (4, 2)):
            if n < zs:
                @pl.when(i == at_end)
                def _():
                    land(n)

        return carry

    spread_at = [min(n, zs - 1) for n in (2, 2, 3)]
    hop_at = [min(n, zs - 1) for n in (4, 5, 6)]
    lax.fori_loop(0, zs, step, 0)
    middle(zs - 1)
    conv_x[0].start()
    conv_x[2].start()
    finish(zs - 2)
    finish(zs - 1)
    conv_x[1].start()
    for k in (1, 3, 2):
        w_share(k)

    returned[mine, :] = back_out[mine, :]
    def combine(c):
        here = slice(c * chunk + (0 if c else cap), (c + 1) * chunk)
        received(returned.at[here, :], back_recv.at[c])
        return jnp.dot(scale[c], returned[c * chunk : (c + 1) * chunk, :], preferred_element_type=f32)

    total = combine(0)
    for c in range(1, zs - 1):
        total = total + combine(c)
    running[...] = total
    total = running[...] + combine(zs - 1)
    combined[...] = total.astype(bf16)
    last = []
    for k in range(1, 4):
        to = lax.rem(me + k, 4)
        last.append(
            remote(
                combined.at[aligned(to * rows, rows), :], final.at[me],
                fin_send, fin_recv, {"tp": to},
            )
        )
    for r in last:
        r.start()
    final[me] = combined[aligned(me * rows, rows), :]
    received(xin.at[0], cx_recv.at[0])
    received(xin.at[0], cx_recv.at[2])
    if cs > 1:
        received(wfull.at[0:xs, 0:3], wd_recv)
    lax.fori_loop(0, per, multiply, 0)
    received(xin.at[0], cx_recv.at[1])
    lax.fori_loop(0, per, multiply_last, 0)
    received(final.at[0:3], fin_recv)
    for b in range(4):
        moe_out[:, b * col : (b + 1) * col] = final[b]

    gone(own.at[0:6], a2a_send)
    gone(xin.at[0:3], cx_send)
    gone(stats_in, stat_send)
    hist.wait_send()
    gone(wfull.at[0, 0:3, 0:own_rows], wy_send)
    gone(wfull.at[0, 0:3, 0:own_rows], wz_send)
    gone(wfull.at[0 : xs - 1, 0:3], wx_send)
    if cs > 1:
        gone(wfull.at[0:xs, 0:3], wd_send)
    sent = (2 * (zs - far_to + far_from) + far_to - far_from) * chunk // 2 - cap
    gone(outgoing.at[:, 0:sent, :], ep_send)
    gone(arrived.at[0], gather_send.at[0])
    gone(arrived.at[0], gather_send.at[1])
    if far_to > far_from:
        gone(arrived.at[0, 0 : (far_to - far_from) * chunk], gather_send.at[2])
    gone(moe_a, ret_send.at[0])
    gone(moe_b, ret_send.at[1])
    gone(moe_c, ret_send.at[2])
    gone(moe_d, ret_send.at[3])
    gone(back_out.at[cap:, :], back_send)
    gone(final.at[0:3], fin_send)


def local(
    conv_input, conv_kernel, norm_gain, norm_shift, conv_proj, moe_input, moe_gain,
    routes, route_weights, gate_proj, up_proj, down_proj, *, dims=DIMS,
):
    zs, xs, cs = dims
    ep_count = zs * xs * cs
    conv_rows, conv_width = conv_input.shape
    rows, width = moe_input.shape
    group_rows = routes.shape[0]
    cap = 16
    slots = ep_count * cap
    col, half = width // 4, width // 8
    span = conv_rows // 4
    hid = gate_proj.shape[2]
    chunk = xs * cs * cap
    per = xs * cs
    vmem, dma = pltpu.VMEM, pltpu.SemaphoreType.DMA
    at_vmem, at_hbm = pl.BlockSpec(memory_space=pltpu.VMEM), pl.BlockSpec(memory_space=pltpu.HBM)
    scratch = [
        vmem((32 + conv_rows, conv_width), bf16),
        vmem((32, conv_width), bf16),
        vmem((32, conv_width), f32),
        vmem((conv_rows, conv_width), f32),
        vmem((2, span // 2, 128), f32),
        vmem((2, 8, span // 2), f32),
        vmem((3, 2, 8, span // 2), f32),
        vmem((conv_rows, 8), f32),
        vmem((conv_rows, conv_width), bf16),
        vmem((4, span, conv_width), bf16),
        vmem((per, span, width // per), f32),
        vmem((per, 4, conv_width, width // per), bf16),
        vmem((4, col, hid), bf16), vmem((4, col, hid), bf16), vmem((4, hid, col), bf16),
        vmem((6, rows, col), bf16),
        vmem((2, group_rows, col), bf16),
        vmem((ep_count, group_rows), f32), vmem((ep_count, group_rows), f32),
        vmem((zs, group_rows, chunk), bf16),
        vmem((2, slots, col), bf16),
        vmem((4, slots, col), bf16),
        vmem((4, slots, col), bf16),
        vmem((slots, half), bf16), vmem((slots, half), bf16),
        vmem((slots, col), bf16), vmem((slots, col), bf16),
        vmem((slots, half), bf16), vmem((slots, half), bf16),
        vmem((slots, col), bf16), vmem((slots, col), bf16),
        vmem((group_rows, col), f32),
        vmem((group_rows, col), bf16),
        vmem((4, rows, col), bf16),
        dma((5,)), pltpu.SemaphoreType.REGULAR,
        dma, dma,
        dma, dma,
        dma, dma((3,)),
        dma, dma,
        dma, dma((3,)),
        dma, dma((3,)),
        dma, dma((3, 3)),
        dma, dma,
        dma, dma((zs,)),
        dma((3,)), dma((3, zs)),
        dma((4,)), dma((4, zs)),
        dma, dma((zs,)),
        dma, dma,
    ]
    return pl.pallas_call(
        functools.partial(layer, dims=dims, cap=cap),
        out_shape=(
            jax.ShapeDtypeStruct((span, width), bf16),
            jax.ShapeDtypeStruct((rows, width), bf16),
        ),
        in_specs=[at_vmem] * 7 + [at_hbm] * 5,
        out_specs=(at_vmem, at_vmem),
        scratch_shapes=scratch,
        compiler_params=pltpu.CompilerParams(
            collective_id=0, has_side_effects=True, vmem_limit_bytes=60 * 1024 * 1024
        ),
    )(
        moe_input, moe_gain[None, :], routes.T, route_weights.T, conv_kernel, norm_gain[None, :],
        norm_shift[None, :], conv_input, conv_proj, gate_proj, up_proj, down_proj,
    )


def solution(mesh):
    placed = (
        P("ep", "tp"),
        P(None, "tp"),
        P("tp"),
        P("tp"),
        P("tp", None),
        P(("ep", "tp"), None),
        P(),
        P("ep", None),
        P("ep", None),
        P("ep", None, "tp"),
        P("ep", None, "tp"),
        P("ep", "tp", None),
    )
    return jax.shard_map(
        local,
        mesh=mesh,
        in_specs=placed,
        out_specs=(P(("ep", "tp"), None), P(("ep", "tp"), None)),
        check_vma=False,
    )
```

```python
import functools

import jax
import jax.numpy as jnp
from jax import lax
from jax.experimental import pallas as pl
from jax.experimental.pallas import tpu as pltpu
from jax.sharding import PartitionSpec as P

MESH = pl.DeviceIdType.MESH
DIMS = (8, 4, 2)
OFFSETS = {8: (0, 3, 5, 4, 2, 6, 1, 7), 4: (0, 2, 1, 3), 2: (0, 1)}
FAR = {8: (1, 4), 4: (1, 2), 2: (2, 2)}
ISSUE = {8: ((0,), (1, 2), (3,), (4, 5), (6, 7)), 4: ((0,), (1,), (2, 3)), 2: ((0,), (1,))}
f32, bf16, i32 = jnp.float32, jnp.bfloat16, jnp.int32


def layer(
    moe_in_hbm, moe_gain_hbm, routes_hbm, weights_hbm, taps_in_hbm, gain_hbm, shift_hbm, conv_hbm, proj_hbm, gate_hbm, up_hbm, down_hbm,
    conv_out, moe_out,
    moe_in, moe_gain, routes, weights, taps_in, gain, shift, padded, history, taps, mixed, sums, stats, stats_in, columns, active, xin, conv_sum, wfull,
    gate, up, down, own, group, ranks, held_w, scale, outgoing, arrived, pieces,
    moe_a, moe_b, moe_c, moe_d, moe_u, moe_v, back_out, returned, running, combined, final,
    load_sem, ready, hist_send, hist_recv, a2a_send, a2a_recv,
    cx_send, cx_recv, stat_send, stat_recv,
    wy_send, wy_recv, wz_send, wz_recv, wx_send, wx_recv, wd_send, wd_recv, ep_send, ep_recv,
    gather_send, gather_recv, ret_send, ret_recv, back_send, back_recv, fin_send, fin_recv,
    *, dims, cap,
):
    zs, xs, cs = dims
    ep_count = zs * xs * cs
    per = xs * cs
    chunk = per * cap
    rows, width = moe_in.shape
    col = width // 4
    half = col // 2
    conv_rows = conv_hbm.shape[0]
    conv_width = conv_hbm.shape[1]
    reach = taps_in.shape[0] - 1
    lead = 32
    span = conv_rows // 4
    slice_cols = width // per

    me_ep, me = lax.axis_index("ep"), lax.axis_index("tp")
    core = lax.rem(me_ep, cs)
    mx = lax.rem(lax.div(me_ep, cs), xs)
    mz = lax.div(me_ep, cs * xs)
    nxt, opp, prv = lax.rem(me + 1, 4), lax.rem(me + 2, 4), lax.rem(me + 3, 4)

    def remote(src, dst, send, recv, where):
        return pltpu.make_async_remote_copy(
            src_ref=src, dst_ref=dst, send_sem=send, recv_sem=recv, device_id=where,
            device_id_type=MESH,
        )

    def received(ref, sem):
        remote(ref, ref, sem, sem, {"tp": lax.rem(me + 1, 4)}).wait_recv()

    def gone(ref, sem):
        remote(ref, ref, sem, sem, {"tp": lax.rem(me + 1, 4)}).wait_send()

    def aligned(start, size):
        return pl.ds(pl.multiple_of(start, size), size)

    offsets = OFFSETS[zs]
    far_from, far_to = FAR[zs]

    def depth(c):
        return offsets[0] + sum(
            (offsets[k] - offsets[k - 1]) * lax.div(c + (zs - k), zs) for k in range(1, zs)
        )

    def place(z, x, c):
        return (z * xs + x) * cs + c

    def partner(c, j, way):
        dx, dc = j // cs, j % cs
        z = lax.rem(mz + way * depth(c) + zs, zs)
        x = lax.rem(mx + way * dx + xs, xs)
        return place(z, x, lax.rem(core + dc, cs))

    barrier = pltpu.get_barrier_semaphore()
    along_z = sorted(range(1, zs), key=lambda d: -min(d, zs - d))
    for d in along_z:
        pl.semaphore_signal(
            barrier, inc=1, device_id={"ep": place(lax.rem(mz + d, zs), mx, core)}, device_id_type=MESH
        )
    for k in (2, 1, 3):
        pl.semaphore_signal(barrier, inc=1, device_id={"tp": lax.rem(me + k, 4)}, device_id_type=MESH)
    for j in range(1, per):
        where = place(mz, lax.rem(mx + j // cs, xs), lax.rem(core + j % cs, cs))
        pl.semaphore_signal(barrier, inc=1, device_id={"ep": where}, device_id_type=MESH)

    loads = [pltpu.make_async_copy(conv_hbm, padded.at[lead:], load_sem.at[0])]
    for q in range(per):
        loads.append(
            pltpu.make_async_copy(
                proj_hbm.at[:, q * slice_cols : (q + 1) * slice_cols], wfull.at[q, me], load_sem.at[1]
            )
        )
    for k in range(4):
        at = lax.rem(me + k, 4) * col
        loads.append(pltpu.make_async_copy(gate_hbm.at[0, aligned(at, col), :], gate.at[k], load_sem.at[2]))
        loads.append(pltpu.make_async_copy(up_hbm.at[0, aligned(at, col), :], up.at[k], load_sem.at[3]))
        loads.append(pltpu.make_async_copy(down_hbm.at[0, :, aligned(at, col)], down.at[k], load_sem.at[4]))
    small = [
        pltpu.make_async_copy(src, dst, load_sem.at[5 + n])
        for n, (src, dst) in enumerate((
            (moe_in_hbm, moe_in), (moe_gain_hbm, moe_gain), (routes_hbm, routes), (weights_hbm, weights),
            (taps_in_hbm, taps_in), (gain_hbm, gain), (shift_hbm, shift),
        ))
    ]
    for load in small + loads:
        load.start()

    def loaded(ref, n):
        pltpu.make_async_copy(ref, ref, load_sem.at[n]).wait()

    for load in small:
        load.wait()
    value = moe_in[...].astype(f32)
    normed = (
        value * lax.rsqrt(jnp.mean(value * value, axis=1, keepdims=True) + 1e-06) * moe_gain[...]
    ).astype(bf16)
    for b in range(5):
        own[b] = normed[:, (b % 4) * col : (b % 4 + 1) * col]

    group_rows = routes.shape[1]
    s_at = lax.broadcasted_iota(i32, (ep_count, group_rows), 0)
    per_bits, core_bits = per.bit_length() - 1, cs.bit_length() - 1
    c_at = s_at >> per_bits
    dz = jnp.full_like(c_at, offsets[0])
    for k in range(1, zs):
        dz = jnp.where(c_at == k, offsets[k], dz)
    dx = (s_at & (per - 1)) >> core_bits
    dc = s_at & (cs - 1)
    expert = ((((mz + dz) & (zs - 1)) * xs + ((mx + dx) & (xs - 1))) * cs) + ((core + dc) & (cs - 1))
    first, second = routes[0:1, :] == expert, routes[1:2, :] == expert
    hit = first | second
    before = (
        lax.broadcasted_iota(i32, (group_rows, group_rows), 0)
        < lax.broadcasted_iota(i32, (group_rows, group_rows), 1)
    )
    rank = jnp.dot(
        jnp.where(hit, 1.0, 0.0).astype(bf16), jnp.where(before, 1.0, 0.0).astype(bf16),
        preferred_element_type=f32,
    )
    ranks[...] = jnp.where(hit, rank, -1.0)
    held_w[...] = jnp.where(first, weights[0:1, :], 0.0) + jnp.where(second, weights[1:2, :], 0.0)
    taps[0 : reach + 1, :] = taps_in[...].astype(f32)

    tile = span // 2
    tiles = conv_rows // tile
    lane, strip = 128, min(64, tile)

    def conv_tile(i, carry):
        for h in range(tile // strip):
            r0 = pl.multiple_of(i * tile + h * strip, strip)
            one = jnp.zeros((strip, lane), f32)
            two = jnp.zeros((strip, lane), f32)
            for n in range(0, conv_width, lane):
                x = padded[pl.ds(r0, strip + lead), n : n + lane].astype(f32)
                out = None
                for phase in range(8):
                    acc = None
                    extra = 8 if phase else 0
                    for q in range(lead // 8 + 1):
                        tap = 8 * q + phase - (lead - reach)
                        if tap < 0 or tap > reach:
                            continue
                        term = x[8 * q : 8 * q + strip + extra] * taps[tap : tap + 1, n : n + lane]
                        acc = term if acc is None else acc + term
                    if acc is None:
                        continue
                    part = acc[phase : phase + strip]
                    out = part if out is None else out + part
                mixed[pl.ds(r0, strip), n : n + lane] = out
                one = one + out
                two = two + out * out
            sums[0, h * strip : (h + 1) * strip, :] = one
            sums[1, h * strip : (h + 1) * strip, :] = two
        for m in range(2):
            stats[m, pl.ds(i, 1), :] = jnp.sum(sums[m].T, axis=0, keepdims=True)
        return carry

    early = tiles * 3 // 8
    loaded(padded.at[lead:], 0)
    lax.fori_loop(1, early, conv_tile, 0)

    pl.semaphore_wait(barrier, zs + per + 1)

    slice_id = mx * cs + core

    own_rows = conv_width // 2
    parity = lax.rem(mz, 2)
    half_rows = own_rows // 2

    def w_first(k):
        piece = wfull.at[slice_id, me, aligned(parity * own_rows, own_rows)]
        return remote(piece, piece, wy_send, wy_recv.at[k - 1], {"tp": lax.rem(me + k, 4)})

    def w_relay(k):
        to, part = (nxt, 0) if k == 1 else (prv, half_rows)
        rows_at = aligned(parity * own_rows + part, half_rows)
        piece = wfull.at[slice_id, lax.rem(me + 4 - k, 4), rows_at]
        return remote(piece, piece, wy_send, wy_recv.at[1], {"tp": to})

    def w_pair(k):
        piece = wfull.at[slice_id, lax.rem(me + 4 - k, 4), aligned(parity * own_rows, own_rows)]
        where = place(mz + 1 - 2 * parity, mx, core)
        return remote(piece, piece, wz_send, wz_recv.at[k - 1], {"ep": where})

    a2a, conv_x, moments = [], [], []
    for k in range(1, 4):
        to = lax.rem(me + k, 4)
        a2a.append(
            remote(
                own.at[pl.ds(to, 2)], group.at[:, aligned(me * rows, rows), :],
                a2a_send, a2a_recv, {"tp": to},
            )
        )
        conv_x.append(
            remote(
                active.at[aligned(to * span, span), :], xin.at[me], cx_send, cx_recv.at[k - 1], {"tp": to},
            )
        )
        moments.append(remote(stats, stats_in.at[k - 1], stat_send, stat_recv, {"tp": to}))
    for r in a2a:
        r.start()
    for d in along_z:
        pl.semaphore_signal(
            ready, inc=1, device_id={"ep": place(lax.rem(mz + d, zs), mx, core)}, device_id_type=MESH
        )
    group[:, aligned(me * rows, rows), :] = own[pl.ds(me, 2)]
    lax.fori_loop(early, tiles * 3 // 4, conv_tile, 0)
    pl.semaphore_wait(ready, zs - 1)
    hist = remote(
        padded.at[conv_rows : conv_rows + lead], history, hist_send, hist_recv,
        {"ep": lax.rem(me_ep + 1, ep_count)},
    )
    hist.start()
    lax.fori_loop(tiles * 3 // 4, tiles, conv_tile, 0)

    def center_and_scale():
        received(stats_in, stat_recv)
        total = (stats[...] + stats_in[0] + stats_in[1] + stats_in[2]) / width
        center = total[0]
        spread = jnp.maximum(total[1] - center * center, 0.0)
        inverse = lax.rsqrt(spread + 1e-05)
        for i in range(tiles):
            both = jnp.concatenate([center[i : i + 1], inverse[i : i + 1]] + [center[i : i + 1]] * 6, axis=0)
            columns[i * tile : (i + 1) * tile, :] = both.T

    def activate(i, carry):
        view = aligned(i * strip, strip)
        stat = columns[view, :]
        scaled = (mixed[view, :] - stat[:, 0:1]) * stat[:, 1:2] * gain[...] + shift[...]
        active[view, :] = (scaled / (1.0 + jnp.exp(-scaled))).astype(bf16)
        return carry

    ends = (1, xs - 1) if xs > 2 else (1,)

    def w_along(k, d):
        piece = wfull.at[slice_id, lax.rem(me + 4 - k, 4)]
        return remote(
            piece, piece, wx_send, wx_recv.at[0 if d == 1 else 1, k - 1],
            {"ep": place(mz, lax.rem(mx + d, xs), core)},
        )

    def w_onward(k, d):
        at = 0 if d == 1 else own_rows
        piece = wfull.at[lax.rem(mx + xs - d, xs) * cs + core, lax.rem(me + 4 - k, 4), at : at + own_rows]
        return remote(
            piece, piece, wx_send, wx_recv.at[2, k - 1],
            {"ep": place(mz, lax.rem(mx + d, xs), core)},
        )

    def w_across(k, d):
        piece = wfull.at[lax.rem(mx + xs - d, xs) * cs + core, lax.rem(me + 4 - k, 4)]
        return remote(
            piece, piece, wd_send, wd_recv,
            {"ep": place(mz, mx, lax.rem(core + 1, cs))},
        )

    def w_spread(k):
        received(wfull.at[0, 0, 0:own_rows], wz_recv.at[k - 1])
        for d in ends:
            w_along(k, d).start()
        if cs > 1:
            w_across(k, 0).start()

    def w_hop(k):
        for n, d in enumerate(ends):
            received(wfull.at[0, 0], wx_recv.at[n, k - 1])
            if xs > 2:
                w_onward(k, d).start()
            if cs > 1:
                w_across(k, d).start()

    def w_share(k):
        if xs > 2:
            received(wfull.at[0, 0], wx_recv.at[2, k - 1])
            if cs > 1:
                w_across(k, 2).start()

    def multiply(q, carry):
        total = sum(
            jnp.dot(xin[b], wfull[q, b], preferred_element_type=f32) for b in (me, prv, nxt)
        )
        conv_sum[q] = total
        return carry

    def multiply_last(q, carry):
        total = conv_sum[q] + jnp.dot(xin[opp], wfull[q, opp], preferred_element_type=f32)
        conv_out[:, aligned(q * slice_cols, slice_cols)] = total.astype(bf16)
        return carry

    received(group.at[:, 0 : 3 * rows, :], a2a_recv)
    loaded(wfull.at[:, 0], 1)
    for k in (1, 3):
        w_first(k).start()

    slot = lax.broadcasted_iota(i32, (cap, group_rows), 0).astype(f32)

    def ep_copy(c, j):
        s = c * per + j
        blocks = slice(0, 1 if far_from <= c < far_to else 2)
        return remote(
            outgoing.at[blocks, aligned(s * cap, cap), :],
            arrived.at[blocks, aligned(s * cap, cap), :],
            ep_send, ep_recv.at[c], {"ep": partner(c, j, 1)},
        )

    def dispatch(group_of):
        for c in group_of:
            ranked = ranks[c * per : (c + 1) * per, :]
            pick = jnp.concatenate(
                [jnp.where(ranked[j : j + 1, :] == slot, 1.0, 0.0) for j in range(per)], axis=0
            ).astype(bf16)
            for b in range(1 if far_from <= c < far_to else 2):
                outgoing[b, c * chunk : (c + 1) * chunk, :] = jnp.dot(
                    pick, group[b], preferred_element_type=f32
                ).astype(bf16)
        for j in range(per):
            for c in group_of:
                if (c, j) != (0, 0):
                    ep_copy(c, j).start()

    for group_of in ISSUE[zs]:
        dispatch(group_of)
    mine = slice(0, cap)
    arrived[0:2, mine, :] = outgoing[:, mine, :]

    hist.wait_recv()
    padded[0:lead, :] = jnp.where(me_ep == 0, jnp.zeros((lead, conv_width), bf16), history[...])
    lax.fori_loop(0, 1, conv_tile, 0)
    for r in moments:
        r.start()

    def weigh(c, carry):
        ranked = ranks[aligned(c * per, per), :]
        held = held_w[aligned(c * per, per), :]
        block = jnp.concatenate(
            [jnp.where(ranked[j : j + 1, :] == slot, held[j : j + 1, :], 0.0) for j in range(per)], axis=0
        )
        scale[c] = block.T.astype(bf16)
        return carry

    lax.fori_loop(0, zs, weigh, 0)

    def is_far(c):
        return (c >= far_from) & (c < far_to)

    def gather_copy(n, c):
        at = aligned(c * chunk, chunk)
        low, high = slice(0, half), slice(half, col)
        src, dst, where = [
            (arrived.at[1, at, :], arrived.at[2, at, :], prv),
            (arrived.at[0, at, :], arrived.at[3, at, :], nxt),
            (arrived.at[0, at, :], arrived.at[1, at, :], prv),
            (arrived.at[1, at, low], arrived.at[2, at, low], prv),
            (arrived.at[3, at, high], arrived.at[2, at, high], nxt),
        ][n]
        sem = (0, 1, 0, 2, 2)[n]
        return remote(src, dst, gather_send.at[sem], gather_recv.at[sem, c], {"tp": where})

    def land(c):
        at = aligned(c * chunk, chunk)

        @pl.when(c == 0)
        def _():
            received(arrived.at[0:2, 0 : chunk - cap, :], ep_recv.at[c])

        @pl.when((c > 0) & jnp.logical_not(is_far(c)))
        def _():
            received(arrived.at[0:2, at, :], ep_recv.at[c])

        @pl.when(is_far(c))
        def _():
            received(arrived.at[0, at, :], ep_recv.at[c])
            gather_copy(2, c).start()

        @pl.when(jnp.logical_not(is_far(c)))
        def _():
            gather_copy(0, c).start()

        gather_copy(1, c).start()

    def relay(c):
        at = aligned(c * chunk, chunk)
        received(arrived.at[1, at, :], gather_recv.at[0, c])
        gather_copy(3, c).start()
        received(arrived.at[3, at, :], gather_recv.at[1, c])
        gather_copy(4, c).start()

    def return_copies(c):
        at = aligned(c * chunk, chunk)
        low, high = slice(0, half), slice(half, col)

        def one(n, src, dst, where):
            return remote(src, dst, ret_send.at[n], ret_recv.at[n, c], {"tp": where})

        return [
            one(0, pieces.at[2, at, low], moe_a.at[at, :], nxt),
            one(1, pieces.at[2, at, high], moe_b.at[at, :], prv),
            one(2, pieces.at[1, at, high], moe_c.at[at, high], nxt),
            one(3, pieces.at[3, at, low], moe_d.at[at, low], prv),
            one(2, moe_u.at[at, :], moe_c.at[at, low], nxt),
            one(3, moe_v.at[at, :], moe_d.at[at, high], prv),
        ]

    def experts(c):
        at = aligned(c * chunk, chunk)

        @pl.when(is_far(c))
        def _():
            received(arrived.at[2, at, :], gather_recv.at[2, c])

        @pl.when(jnp.logical_not(is_far(c)))
        def _():
            received(arrived.at[2, at, :], gather_recv.at[0, c])
            received(arrived.at[3, at, :], gather_recv.at[1, c])

        lines = [arrived[k, at, :] for k in range(4)]
        hidden = []
        step = min(256, col)
        for n in range(0, col, step):
            left = sum(jnp.dot(lines[k], gate[k, :, n : n + step], preferred_element_type=f32) for k in range(4))
            right = sum(jnp.dot(lines[k], up[k, :, n : n + step], preferred_element_type=f32) for k in range(4))
            hidden.append((left / (1.0 + jnp.exp(-left)) * right).astype(bf16))
        hid = jnp.concatenate(hidden, axis=1)
        for k in (2, 1, 3, 0):
            pieces[k, at, :] = jnp.dot(hid, down[k], preferred_element_type=f32).astype(bf16)
        for r in return_copies(c)[:4]:
            r.start()

    def middle(c):
        copies = return_copies(c)
        at = aligned(c * chunk, chunk)
        copies[0].wait_recv()
        moe_u[at, :] = (pieces[1, at, :half].astype(f32) + moe_a[at, :].astype(f32)).astype(bf16)
        copies[4].start()
        copies[1].wait_recv()
        moe_v[at, :] = (pieces[3, at, half:].astype(f32) + moe_b[at, :].astype(f32)).astype(bf16)
        copies[5].start()

    def back_copy(c, j):
        s = c * per + j
        at = aligned(s * cap, cap)
        return remote(
            back_out.at[at, :], returned.at[at, :], back_send, back_recv.at[c],
            {"ep": partner(c, j, -1)},
        )

    def finish(c):
        at = aligned(c * chunk, chunk)
        received(moe_c.at[at, :], ret_recv.at[2, c])
        received(moe_d.at[at, :], ret_recv.at[3, c])
        back_out[at, :] = (
            pieces[0, at, :].astype(f32) + moe_c[at, :].astype(f32) + moe_d[at, :].astype(f32)
        ).astype(bf16)
        for j in range(per):
            if j == 0:
                @pl.when(c > 0)
                def _():
                    back_copy(c, 0).start()
            else:
                back_copy(c, j).start()

    land(0)
    for k in (1, 3):
        received(wfull.at[0, 0, 0:own_rows], wy_recv.at[k - 1])
        w_relay(k).start()
        w_pair(k).start()

    def step(i, carry):
        @pl.when((i >= 3) & (i + 2 < zs))
        def _():
            land(i + 2)

        for n in (1, 2):
            if far_from <= n < far_to:
                @pl.when(i == 1)
                def _():
                    relay(n)

        @pl.when(i == 0)
        def _():
            loaded(gate, 2)
            loaded(up, 3)
            loaded(down, 4)

        experts(i)

        for n in range(max(far_from, 3), far_to):
            @pl.when(i == n - 1)
            def _():
                relay(n)

        @pl.when(i >= 1)
        def _():
            middle(i - 1)

        @pl.when(i >= 2)
        def _():
            finish(i - 2)

        @pl.when(i == 0)
        def _():
            center_and_scale()
            lax.fori_loop(0, conv_rows // strip, activate, 0)
            xin[me] = active[aligned(me * span, span), :]
            received(wfull.at[0, 0, 0:own_rows], wy_recv.at[1])
            w_pair(2).start()

        for n, k in enumerate((1, 3, 2)):
            @pl.when(i == spread_at[n])
            def _():
                w_spread(k)

            @pl.when(i == hop_at[n])
            def _():
                w_hop(k)

        for n, at_end in ((1, 0), (2, 0), (3, 1), (4, 2)):
            if n < zs:
                @pl.when(i == at_end)
                def _():
                    land(n)

        return carry

    spread_at = [min(n, zs - 1) for n in (2, 2, 3)]
    hop_at = [min(n, zs - 1) for n in (4, 5, 6)]
    lax.fori_loop(0, zs, step, 0)
    middle(zs - 1)
    conv_x[0].start()
    conv_x[2].start()
    finish(zs - 2)
    finish(zs - 1)
    conv_x[1].start()
    for k in (1, 3, 2):
        w_share(k)

    returned[mine, :] = back_out[mine, :]
    def combine(c):
        here = slice(c * chunk + (0 if c else cap), (c + 1) * chunk)
        received(returned.at[here, :], back_recv.at[c])
        return jnp.dot(scale[c], returned[c * chunk : (c + 1) * chunk, :], preferred_element_type=f32)

    total = combine(0)
    for c in range(1, zs - 1):
        total = total + combine(c)
    running[...] = total
    total = running[...] + combine(zs - 1)
    combined[...] = total.astype(bf16)
    last = []
    for k in range(1, 4):
        to = lax.rem(me + k, 4)
        last.append(
            remote(
                combined.at[aligned(to * rows, rows), :], final.at[me],
                fin_send, fin_recv, {"tp": to},
            )
        )
    for r in last:
        r.start()
    final[me] = combined[aligned(me * rows, rows), :]
    received(xin.at[0], cx_recv.at[0])
    received(xin.at[0], cx_recv.at[2])
    if cs > 1:
        received(wfull.at[0:xs, 0:3], wd_recv)
    lax.fori_loop(0, per, multiply, 0)
    received(xin.at[0], cx_recv.at[1])
    lax.fori_loop(0, per, multiply_last, 0)
    received(final.at[0:3], fin_recv)
    for b in range(4):
        moe_out[:, b * col : (b + 1) * col] = final[b]

    gone(own.at[0:6], a2a_send)
    gone(xin.at[0:3], cx_send)
    gone(stats_in, stat_send)
    hist.wait_send()
    gone(wfull.at[0, 0:3, 0:own_rows], wy_send)
    gone(wfull.at[0, 0:3, 0:own_rows], wz_send)
    gone(wfull.at[0 : xs - 1, 0:3], wx_send)
    if cs > 1:
        gone(wfull.at[0:xs, 0:3], wd_send)
    sent = (2 * (zs - far_to + far_from) + far_to - far_from) * chunk // 2 - cap
    gone(outgoing.at[:, 0:sent, :], ep_send)
    gone(arrived.at[0], gather_send.at[0])
    gone(arrived.at[0], gather_send.at[1])
    if far_to > far_from:
        gone(arrived.at[0, 0 : (far_to - far_from) * chunk], gather_send.at[2])
    gone(moe_a, ret_send.at[0])
    gone(moe_b, ret_send.at[1])
    gone(moe_c, ret_send.at[2])
    gone(moe_d, ret_send.at[3])
    gone(back_out.at[cap:, :], back_send)
    gone(final.at[0:3], fin_send)


def local(
    conv_input, conv_kernel, norm_gain, norm_shift, conv_proj, moe_input, moe_gain,
    routes, route_weights, gate_proj, up_proj, down_proj, *, dims=DIMS,
):
    zs, xs, cs = dims
    ep_count = zs * xs * cs
    conv_rows, conv_width = conv_input.shape
    rows, width = moe_input.shape
    group_rows = routes.shape[0]
    cap = 16
    slots = ep_count * cap
    col, half = width // 4, width // 8
    span = conv_rows // 4
    hid = gate_proj.shape[2]
    chunk = xs * cs * cap
    per = xs * cs
    reach = conv_kernel.shape[0] - 1
    vmem, dma = pltpu.VMEM, pltpu.SemaphoreType.DMA
    at_vmem, at_hbm = pl.BlockSpec(memory_space=pltpu.VMEM), pl.BlockSpec(memory_space=pltpu.HBM)
    scratch = [
        vmem((rows, width), bf16), vmem((1, width), f32), vmem((2, group_rows), i32), vmem((2, group_rows), f32),
        vmem((reach + 1, conv_width), bf16), vmem((1, conv_width), f32), vmem((1, conv_width), f32),
        vmem((32 + conv_rows, conv_width), bf16),
        vmem((32, conv_width), bf16),
        vmem((32, conv_width), f32),
        vmem((conv_rows, conv_width), f32),
        vmem((2, span // 2, 128), f32),
        vmem((2, 8, span // 2), f32),
        vmem((3, 2, 8, span // 2), f32),
        vmem((conv_rows, 8), f32),
        vmem((conv_rows, conv_width), bf16),
        vmem((4, span, conv_width), bf16),
        vmem((per, span, width // per), f32),
        vmem((per, 4, conv_width, width // per), bf16),
        vmem((4, col, hid), bf16), vmem((4, col, hid), bf16), vmem((4, hid, col), bf16),
        vmem((6, rows, col), bf16),
        vmem((2, group_rows, col), bf16),
        vmem((ep_count, group_rows), f32), vmem((ep_count, group_rows), f32),
        vmem((zs, group_rows, chunk), bf16),
        vmem((2, slots, col), bf16),
        vmem((4, slots, col), bf16),
        vmem((4, slots, col), bf16),
        vmem((slots, half), bf16), vmem((slots, half), bf16),
        vmem((slots, col), bf16), vmem((slots, col), bf16),
        vmem((slots, half), bf16), vmem((slots, half), bf16),
        vmem((slots, col), bf16), vmem((slots, col), bf16),
        vmem((group_rows, col), f32),
        vmem((group_rows, col), bf16),
        vmem((4, rows, col), bf16),
        dma((12,)), pltpu.SemaphoreType.REGULAR,
        dma, dma,
        dma, dma,
        dma, dma((3,)),
        dma, dma,
        dma, dma((3,)),
        dma, dma((3,)),
        dma, dma((3, 3)),
        dma, dma,
        dma, dma((zs,)),
        dma((3,)), dma((3, zs)),
        dma((4,)), dma((4, zs)),
        dma, dma((zs,)),
        dma, dma,
    ]
    return pl.pallas_call(
        functools.partial(layer, dims=dims, cap=cap),
        out_shape=(
            jax.ShapeDtypeStruct((span, width), bf16),
            jax.ShapeDtypeStruct((rows, width), bf16),
        ),
        in_specs=[at_hbm] * 12,
        out_specs=(at_vmem, at_vmem),
        scratch_shapes=scratch,
        compiler_params=pltpu.CompilerParams(
            collective_id=0, has_side_effects=True, vmem_limit_bytes=60 * 1024 * 1024
        ),
    )(
        moe_input, moe_gain[None, :], routes.T, route_weights.T, conv_kernel, norm_gain[None, :],
        norm_shift[None, :], conv_input, conv_proj, gate_proj, up_proj, down_proj,
    )


def solution(mesh):
    placed = (
        P("ep", "tp"),
        P(None, "tp"),
        P("tp"),
        P("tp"),
        P("tp", None),
        P(("ep", "tp"), None),
        P(),
        P("ep", None),
        P("ep", None),
        P("ep", None, "tp"),
        P("ep", None, "tp"),
        P("ep", "tp", None),
    )
    return jax.shard_map(
        local,
        mesh=mesh,
        in_specs=placed,
        out_specs=(P(("ep", "tp"), None), P(("ep", "tp"), None)),
        check_vma=False,
    )
```
